32 devices in a mesh: ep: 8 (over z, core), tp: 4 (over y, x).
Axes of the slice: x: 2, y: 2, z: 4, core: 2. Of those that a mesh axis runs over, the one named last changes fastest.
Arguments:
- mix_in: bfloat16 [2048, 2048], P('ep'), may hold values from -6 to 6
- mix_gain: float32 [2048], replicated, may hold values from 0.1 to 1.9
- w_in_x: bfloat16 [2048, 2048], P(None, 'tp'), may hold values from -0.125 to 0.125
- w_in_y: bfloat16 [2048, 2048], P(None, 'tp'), may hold values from -0.125 to 0.125
- conv_taps: float32 [4, 2048], P(None, 'tp'), may hold values from -3 to 3
- recur_gate_w: bfloat16 [16, 128, 128], P('tp'), may hold values from -0.5 to 0.5
- input_gate_w: bfloat16 [16, 128, 128], P('tp'), may hold values from -0.5 to 0.5
- decay_logit: float32 [2048], P('tp'), may hold values from 4 to 20
- decay_shift: float32 [2048, 2048], P('ep', 'tp'), may hold values from -2.2 to 0
- moe_in: bfloat16 [2048, 2048], P('ep'), may hold values from -6 to 6
- moe_gain: float32 [2048], replicated, may hold values from 0.1 to 1.9
- routes: int32 [2048, 2], P('ep'), may hold values from 0 to 7, all different within a row; in each aligned block of 256 rows (0 to 255, 256 to 511, ...) at most 128 rows name the same one
- route_weight: float32 [2048, 2], P('ep'), may hold values from 0.1 to 1
- expert_gate: bfloat16 [8, 2048, 2048], P('ep', None, 'tp'), may hold values from -0.125 to 0.125
- expert_up: bfloat16 [8, 2048, 2048], P('ep', None, 'tp'), may hold values from -0.125 to 0.125
- expert_down: bfloat16 [8, 2048, 2048], P('ep', None, 'tp'), may hold values from -0.125 to 0.125
Outputs:
- mixer_out: bfloat16 [2048, 2048], P('ep', 'tp')
- moe_out: bfloat16 [2048, 2048], P('ep', 'tp')
The draws below stay inside these ranges and needn't reach their ends.
Inputs may be any that keep to these rules, and one draw needn't show every extreme that they name: `routes`: each row names 2 different experts. Among the rows of one index of ep no expert is named more than 128 times, a bound that some block reaches.
All inputs are finite; a program needn't handle non-finite values.
Results may differ from the reference program's by a relative error of at most 0.0095.
Values may be sent and summed in bfloat16 or wider, within the bound.
A program may use at most 64 MiB of HBM per device.

```python
import math
import jax
import jax.numpy as jnp
import numpy as np
from jax import lax

D = 2048
FILTER_SECTIONS = 16
SECTION_FEATURES = 128
KCONV = 4
FF = 2048
TOPK = 2
TOK_DEV = 256
SUBBATCH_SPAN = 2048
WIDTH = 2048
EXPERTS = 8
CAP = 128
N_EP = 8


def draw_decay_logit(key, part):
    pick_key, slow_key, fast_key, jitter_key = jax.random.split(jax.random.fold_in(key, 11), 4)
    fast_head = jax.random.uniform(pick_key, (FILTER_SECTIONS,)) < 0.5
    slow_rate = jnp.exp(jax.random.uniform(slow_key, (FILTER_SECTIONS,), minval=math.log(0.2), maxval=math.log(0.6))) / SUBBATCH_SPAN
    fast_rate = jnp.exp(jax.random.uniform(fast_key, (FILTER_SECTIONS,), minval=math.log(0.01), maxval=math.log(1.0 / 30.0)))
    head_rate = jnp.where(fast_head, fast_rate, slow_rate)
    jitter = jax.random.uniform(jitter_key, (FILTER_SECTIONS, SECTION_FEATURES), minval=0.7, maxval=1.4)
    softened = (head_rate[:, None] * jitter / 4.0).reshape(FILTER_SECTIONS * SECTION_FEATURES)
    return -jnp.log(jnp.expm1(softened))


def draw_decay_shift(key, part):
    block_key, chan_key, place_key, depth_key = jax.random.split(jax.random.fold_in(key, 23), 4)
    blocks = SUBBATCH_SPAN // TOK_DEV
    spread = math.log(2.0)
    factor = jnp.exp(jax.random.uniform(block_key, (blocks,), minval=-spread, maxval=spread))
    channel = jax.random.uniform(chan_key, (FILTER_SECTIONS * SECTION_FEATURES,), minval=0.2, maxval=0.8)
    stationary_regime = -jnp.repeat(factor, TOK_DEV)[:, None] * channel[None, :] / SUBBATCH_SPAN
    assignment_seats = jax.random.randint(place_key, (3, FILTER_SECTIONS), 0, SUBBATCH_SPAN)
    stack_levels = jnp.log1p(-jax.random.uniform(depth_key, (3, FILTER_SECTIONS), minval=0.2, maxval=0.5))
    sequence_offsets = jnp.arange(SUBBATCH_SPAN)[:, None]
    packet_clusters = jnp.zeros((SUBBATCH_SPAN, FILTER_SECTIONS), jnp.float32)
    for picked_ordinal in range(3):
        packet_clusters = packet_clusters + jnp.where(sequence_offsets == assignment_seats[picked_ordinal][None, :], stack_levels[picked_ordinal][None, :], 0.0)
    return stationary_regime + jnp.repeat(packet_clusters, SECTION_FEATURES, axis=1)


def shard_levels(rng, shape, shards, least, high):
    factor_of = 1.0
    for axis_at, parts in shards:
        heights = jax.random.uniform(jax.random.fold_in(jax.random.fold_in(rng, 6), axis_at), (parts,), jnp.float32, least / len(shards), high / len(shards))
        factor_of = factor_of * jnp.repeat(jnp.exp(heights), shape[axis_at] // parts).reshape((-1,) + (1,) * (len(shape) - 1 - axis_at))
    return factor_of


def assign_block(rng, own, number, rows, amount, top, most, skew):
    sequence = jax.random.permutation(rng, amount)
    crowded, common = load_shares(amount, rows * top, most, skew, True), load_shares(amount, rows * top, most, skew, False)
    places = jnp.arange(amount)

    def named(sizes, offset_by):
        used = int((sizes > 0).sum())
        fixed = max(1, used // 4)
        passed = fixed + (places - fixed + offset_by * (used - fixed)) % max(1, amount - fixed)
        return jnp.zeros((amount,), jnp.int32).at[sequence[jnp.where(places < fixed, places, passed)]].set(jnp.asarray(sizes, jnp.int32))

    sizes = jnp.where(number % 4 == 0, named(crowded, number // 4), named(common, number - number // 4 - 1))
    mixed = jax.random.permutation(jax.random.fold_in(own, 3), amount)
    giver, taker = mixed[0:amount // 2 * 2:2], mixed[1:amount // 2 * 2:2]
    slack = jnp.minimum(sizes[giver] - 1, most - sizes[taker]) // 2
    slack = jnp.where((giver == sequence[0]) | (taker == sequence[0]) | (sizes[taker] == 0), 0, jnp.maximum(slack, 0))
    passed = jax.random.randint(jax.random.fold_in(own, 4), (amount // 2,), 0, 1 << 20) % (slack + 1)
    sizes = sizes.at[giver].add(-passed).at[taker].add(passed)
    labels = jnp.searchsorted(jnp.cumsum(sizes), jnp.arange(rows * top), side="right").astype(jnp.int32)
    listing = labels.reshape(top, rows).T
    listing = listing[jax.random.permutation(jax.random.fold_in(own, 1), rows)]
    offset_by = jax.random.randint(jax.random.fold_in(own, 2), (rows, 1), 0, top)
    return jnp.take_along_axis(listing, (jnp.arange(top)[None, :] + offset_by) % top, axis=1)


def load_shares(number_of, total, most, slope, full):
    portions = [(1 << 20) // math.isqrt(grade ** slope) + 1 for grade in range(1, number_of + 1)]
    largest = most if full else min(most, max(-(-total // number_of), total * portions[0] // sum(portions)))
    least = 1 if total - largest >= number_of - 1 else 0
    holding, spare = [largest] + [least] * (number_of - 1), total - largest - least * (number_of - 1)
    while spare > 0:
        free = [i for i in range(1, number_of) if holding[i] < largest] or [i for i in range(1, number_of) if holding[i] < most]
        mass, remaining = sum([portions[i] for i in free]), spare
        for i in free:
            more = min(most - holding[i], max(1, remaining * portions[i] // mass), spare)
            holding[i] = holding[i] + more
            spare = spare - more
    return np.array(holding)


def noise(rng, shape, scale, bound, shards=(), held_as=jnp.bfloat16):
    level = shard_levels(rng, shape, shards, -0.22, 0.18) if shards else 1.0
    drawn = jax.random.normal(rng, shape, jnp.float32) * scale * level
    return jnp.minimum(jnp.maximum(drawn, -bound), bound).astype(held_as)


def setup_inputs(seed: int = 0) -> dict:
    keys = jax.random.split(jax.random.key(seed), 17)
    mix_in = noise(keys[0], (SUBBATCH_SPAN, D), 1.0, 6.0, ((0, 8),))
    mix_gain = jnp.clip(1.0 + 0.18 * jax.random.normal(keys[1], (D,), jnp.float32), 0.1, 1.9)
    w_in_x = noise(keys[2], (D, WIDTH), D ** -0.5, 0.125, ((1, 4),))
    w_in_y = noise(keys[3], (D, WIDTH), D ** -0.5, 0.125, ((1, 4),))
    conv_taps = noise(keys[4], (KCONV, WIDTH), 0.5, 3.0, ((1, 4),), jnp.float32)
    recur_gate_w = noise(keys[5], (FILTER_SECTIONS, SECTION_FEATURES, SECTION_FEATURES), SECTION_FEATURES ** -0.5, 0.5, ((0, 4),))
    input_gate_w = noise(keys[6], (FILTER_SECTIONS, SECTION_FEATURES, SECTION_FEATURES), SECTION_FEATURES ** -0.5, 0.5, ((0, 4),))
    decay_logit = draw_decay_logit(jax.random.fold_in(keys[16], 71), 0)
    decay_shift = draw_decay_shift(jax.random.fold_in(keys[16], 71), 0)
    moe_in = noise(keys[9], (SUBBATCH_SPAN, D), 1.0, 6.0, ((0, 8),))
    moe_gain = jnp.clip(1.0 + 0.18 * jax.random.normal(keys[10], (D,), jnp.float32), 0.1, 1.9)
    routes_keys = jax.random.split(jax.random.fold_in(keys[11], 1), SUBBATCH_SPAN // TOK_DEV)
    routes_turns = jax.random.permutation(jax.random.fold_in(keys[11], 3), SUBBATCH_SPAN // TOK_DEV)
    routes = jax.vmap(lambda own, number: assign_block(jax.random.fold_in(keys[11], 2), own, number, TOK_DEV, EXPERTS, TOPK, CAP, 2))(routes_keys, routes_turns).reshape((SUBBATCH_SPAN, TOPK))
    route_weight = jnp.clip(jnp.exp(math.log(1.0) - 2.3025851 * jax.random.uniform(keys[12], (SUBBATCH_SPAN, TOPK), jnp.float32) ** shard_levels(keys[12], (SUBBATCH_SPAN, TOPK), ((0, 8),), -0.2, 0.2)), 0.1, 1.0)
    expert_gate = noise(keys[13], (EXPERTS, D, FF), D ** -0.5, 0.125, ((0, 8), (2, 4)))
    expert_up = noise(keys[14], (EXPERTS, D, FF), D ** -0.5, 0.125, ((0, 8), (2, 4)))
    expert_down = noise(keys[15], (EXPERTS, FF, D), FF ** -0.5, 0.125, ((0, 8), (2, 4)))
    return {"mix_in": mix_in, "mix_gain": mix_gain, "w_in_x": w_in_x, "w_in_y": w_in_y, "conv_taps": conv_taps, "recur_gate_w": recur_gate_w, "input_gate_w": input_gate_w, "decay_logit": decay_logit, "decay_shift": decay_shift, "moe_in": moe_in, "moe_gain": moe_gain, "routes": routes, "route_weight": route_weight, "expert_gate": expert_gate, "expert_up": expert_up, "expert_down": expert_down}


epsilon = 1e-06
lru_scale = 8.0

def norm_rows(rows, gain):
    widened = rows.astype(jnp.float32)
    scaled = widened * lax.rsqrt(lax.optimization_barrier(jnp.mean(widened * widened, axis=-1, keepdims=True)) + epsilon)
    return (scaled * gain.astype(jnp.float32)[None, :]).astype(jnp.bfloat16)

def link(earlier, later):
    return (earlier[0] * later[0], later[0] * earlier[1] + later[1])

def reference(mix_in, mix_gain, w_in_x, w_in_y, conv_taps, recur_gate_w, input_gate_w, decay_logit, decay_shift, moe_in, moe_gain, routes, route_weight, expert_gate, expert_up, expert_down):
    mixer_rows = norm_rows(mix_in, mix_gain)
    x_branch = jnp.dot(mixer_rows, w_in_x, preferred_element_type=jnp.float32).astype(jnp.bfloat16)
    y_branch = jnp.dot(mixer_rows, w_in_y, preferred_element_type=jnp.float32).astype(jnp.bfloat16)
    padded = jnp.concatenate([jnp.zeros((KCONV - 1, WIDTH), jnp.bfloat16), x_branch], axis=0)
    conv_sum = jnp.zeros((SUBBATCH_SPAN, WIDTH), jnp.float32)
    for tap_index in range(KCONV):
        conv_sum = conv_sum + conv_taps[tap_index][None, :].astype(jnp.float32) * padded[tap_index:tap_index + SUBBATCH_SPAN].astype(jnp.float32)
    x_conv = conv_sum.astype(jnp.bfloat16)
    heads_in = x_conv.astype(jnp.float32).reshape(SUBBATCH_SPAN, FILTER_SECTIONS, SECTION_FEATURES)
    gate_a = jnp.einsum('thi,hij->thj', heads_in, recur_gate_w.astype(jnp.float32)).reshape(SUBBATCH_SPAN, WIDTH)
    gate_x = jnp.einsum('thi,hij->thj', heads_in, input_gate_w.astype(jnp.float32)).reshape(SUBBATCH_SPAN, WIDTH)
    log_decay = -lru_scale * jax.nn.sigmoid(gate_a) * jax.nn.softplus(-decay_logit)[None, :] + decay_shift
    lru_drive = jnp.sqrt(-jnp.expm1(2.0 * log_decay)) * jax.nn.sigmoid(gate_x) * x_conv.astype(jnp.float32)
    through, lru_state = lax.associative_scan(link, (jnp.exp(log_decay), lru_drive), axis=0)
    mixer_out = (lru_state * jax.nn.gelu(y_branch.astype(jnp.float32))).astype(jnp.bfloat16)
    moe_rows = norm_rows(moe_in, moe_gain)
    grouped = routes.reshape(N_EP, TOK_DEV * TOPK)
    onehot = (grouped[:, :, None] == jnp.arange(EXPERTS, dtype=jnp.int32)[None, None, :]).astype(jnp.int32)
    slot_rank = lax.optimization_barrier(jnp.sum(jnp.cumsum(onehot, axis=1) * onehot, axis=2)) - 1
    source = jnp.broadcast_to(jnp.arange(N_EP, dtype=jnp.int32)[:, None], slot_rank.shape)
    slot_index = (source * CAP + slot_rank).reshape(-1).astype(jnp.int32)
    expert_ids = routes.reshape(-1).astype(jnp.int32)
    token_index = jnp.repeat(jnp.arange(SUBBATCH_SPAN, dtype=jnp.int32), TOPK)
    table = jnp.zeros((EXPERTS, N_EP * CAP, D), jnp.bfloat16).at[expert_ids, slot_index].set(moe_rows[token_index])

    def run_expert(packed):
        rows_in, gate_w, up_w, down_w = packed
        gate_proj = jnp.dot(rows_in, gate_w, preferred_element_type=jnp.float32)
        up_proj = jnp.dot(rows_in, up_w, preferred_element_type=jnp.float32)
        hidden = (jax.nn.silu(gate_proj) * up_proj).astype(jnp.bfloat16)
        return jnp.dot(hidden, down_w, preferred_element_type=jnp.float32).astype(jnp.bfloat16)
    results = lax.map(run_expert, (table, expert_gate, expert_up, expert_down))
    picked = results[expert_ids, slot_index].astype(jnp.float32).reshape(SUBBATCH_SPAN, TOPK, D)
    route_share = route_weight / lax.optimization_barrier(jnp.sum(route_weight, axis=1, keepdims=True))
    moe_out = lax.optimization_barrier(jnp.sum(route_share[:, :, None] * picked, axis=1)).astype(jnp.bfloat16)
    return (mixer_out, moe_out)
```

```python
import functools

import jax
import jax.numpy as jnp
from jax import lax
from jax.experimental import pallas as pl
from jax.experimental.pallas import tpu as pltpu
from jax.sharding import PartitionSpec as P

epsilon = 1e-06
lru_scale = 8.0
MESH = pl.DeviceIdType.MESH
F32 = jnp.float32
BF16 = jnp.bfloat16


block_order = ((1, 2, 3), (0, 3, 2), (3, 0, 1), (2, 1, 0))


def one_minus_exp(value):
    series = jnp.full_like(value, 1.0 / 9.0)
    for k in range(8, 1, -1):
        series = (1.0 + value * series) * (1.0 / k)
    series = 1.0 + value * series
    return jnp.where(value > -0.5, -value * series, 1.0 - jnp.exp(value))


def soft_plus(value):
    small = jnp.exp(-jnp.abs(value))
    series = jnp.full_like(small, 1.0 / 7.0)
    for k in range(6, 0, -1):
        series = 1.0 / k - small * series
    wide = jnp.where(small < 0.05, small * series, jnp.log(1.0 + small))
    return jnp.maximum(value, 0.0) + wide


def both_kernel(
    cap,
    mix_hbm,
    wx_hbm,
    wy_hbm,
    ga_hbm,
    gx_hbm,
    shift_hbm,
    mix_gain_ref,
    taps_ref,
    logit_ref,
    moe_hbm,
    gain_ref,
    rt_row,
    rw_row,
    gate_hbm,
    up_hbm,
    down_hbm,
    mix_ref,
    out_ref,
    nrm,
    tok,
    xs,
    stage,
    own_stage,
    picks,
    hid,
    psend,
    precv,
    pown,
    res,
    ret,
    routes_all,
    comb,
    part,
    total,
    gw,
    uw,
    w2,
    load_sem,
    rt_sem,
    z_send,
    z_recv,
    w_sem,
    x_send,
    x_recv,
    ag_sem,
    rs_sem,
    ret_sem,
    mixv,
    wx,
    wy,
    gaw,
    gxw,
    shiftv,
    xb,
    yb,
    av,
    bv,
    ends,
    halo_sem,
    ends_sem,
):
    n_ep = lax.axis_size("ep")
    nz = n_ep // 2
    ep = lax.axis_index("ep")
    t = lax.axis_index("tp")
    z, c = ep // 2, ep % 2
    y, x = t // 2, t % 2
    xp, yp, dg = y * 2 + (1 - x), (1 - y) * 2 + x, 3 - t
    pa, pb = jnp.where(c == 0, xp, yp), jnp.where(c == 0, yp, xp)
    other = z * 2 + (1 - c)
    rows, share = tok.shape[2], tok.shape[3]
    inner = (z > 0) & (z + 1 < nz)

    def block_at(s):
        q = jnp.int32(0)
        for zz in range(nz):
            q = jnp.where(z == zz, block_order[zz][s], q)
        return q

    def remote(src, dst, send, recv, where):
        return pltpu.make_async_remote_copy(
            src_ref=src,
            dst_ref=dst,
            send_sem=send,
            recv_sem=recv,
            device_id=where,
            device_id_type=MESH,
        )

    span = w2.shape[2]
    half = w2.shape[1] // 2

    def down_rows(k):
        return down_hbm.at[0, pl.ds(pl.multiple_of(k * half, half), half)]

    loads = [
        pltpu.make_async_copy(moe_hbm, nrm, load_sem.at[0]),
        pltpu.make_async_copy(gate_hbm.at[0], gw, load_sem.at[1]),
        pltpu.make_async_copy(up_hbm.at[0], uw, load_sem.at[2]),
        pltpu.make_async_copy(mix_hbm, mixv, load_sem.at[3]),
        pltpu.make_async_copy(wx_hbm, wx, load_sem.at[4]),
        pltpu.make_async_copy(wy_hbm, wy, load_sem.at[5]),
        pltpu.make_async_copy(ga_hbm, gaw, load_sem.at[6]),
        pltpu.make_async_copy(gx_hbm, gxw, load_sem.at[7]),
        pltpu.make_async_copy(shift_hbm, shiftv, load_sem.at[8]),
        pltpu.make_async_copy(down_rows(t), w2.at[0, pl.ds(0, half)], load_sem.at[9]),
        pltpu.make_async_copy(down_rows(pa), w2.at[0, pl.ds(half, half)], load_sem.at[10]),
    ]
    loads[0].start()
    barrier = pltpu.get_barrier_semaphore()
    for by in range(1, n_ep):
        pl.semaphore_signal(
            barrier, inc=1, device_id={"ep": (ep + by) % n_ep}, device_id_type=MESH
        )
    for peer in (xp, yp):
        for near in (ep, other):
            pl.semaphore_signal(
                barrier, inc=1, device_id={"ep": near, "tp": peer}, device_id_type=MESH
            )
    for copy in loads[3:6] + loads[1:3] + loads[6:]:
        copy.start()

    def columns(k):
        return pl.ds(pl.multiple_of(k * share, share), share)

    def z_own(k, up):
        return remote(
            nrm.at[:, columns((t, dg)[k])],
            tok.at[z, k],
            z_send.at[up, k, z],
            z_recv.at[k, z],
            {"ep": ep + (2 if up else -2)},
        )

    def z_copy(q, k, up):
        return remote(
            tok.at[q, k],
            tok.at[q, k],
            z_send.at[up, k, q],
            z_recv.at[k, q],
            {"ep": ep + (2 if up else -2)},
        )

    def route_copy(q):
        return remote(rt_row, routes_all.at[z], rt_sem.at[0, q], rt_sem.at[1, z], {"ep": q * 2 + c})

    def w_copy(k):
        piece = half // 2
        first = (pb, dg)[k // 2] * half + k % 2 * piece
        return remote(
            down_hbm.at[0, pl.ds(pl.multiple_of(first, piece), piece)],
            w2.at[1, pl.ds(k * piece, piece)],
            w_sem.at[0, k],
            w_sem.at[1, k],
            {"tp": pb},
        )

    def xs_part(q, block, k):
        return xs.at[q, pl.ds(pl.multiple_of(block * cap, cap), cap), columns(k)]

    def x_copy(q, kind):
        to = (xp, yp, xp, yp, t, t)[kind]
        near = ep if kind < 2 else other
        src = xs_part(q, c, t) if kind < 2 else stage.at[q, kind // 5]
        return remote(
            src,
            xs_part(q, c, dg if kind == 5 else t),
            x_send.at[kind, q],
            x_recv.at[kind, q],
            {"ep": near, "tp": to},
        )

    def x_wait(q, kind):
        block = c if kind < 2 else 1 - c
        dst = xs_part(q, block, (xp, yp, xp, yp, t, dg)[kind])
        remote(
            stage.at[q, 0], dst, x_send.at[kind, q], x_recv.at[kind, q], {"ep": other}
        ).wait_recv()

    def own_copy(block):
        return remote(
            own_stage,
            xs.at[z, pl.ds(pl.multiple_of(block * cap, cap), cap)],
            x_send.at[4, z],
            x_recv.at[4, z],
            {"ep": other},
        )

    def ag_copy(q, cc):
        at, sem = pl.ds(cc * cap, cap), q * 2 + cc
        return remote(
            hid.at[q, at, pl.ds(0, half)],
            hid.at[q, at, pl.ds(half, half)],
            ag_sem.at[0, sem],
            ag_sem.at[1, sem],
            {"tp": pa},
        )

    def rs_copy(q, cc):
        at, sem = pl.ds(cc * cap, cap), q * 2 + cc
        return remote(
            psend.at[q, at], precv.at[q, at], rs_sem.at[0, sem], rs_sem.at[1, sem], {"tp": pb}
        )

    def ret_copy(q, cc):
        return remote(
            res.at[q, pl.ds(cc * cap, cap)],
            ret.at[ep],
            ret_sem.at[0, q * 2 + cc],
            ret_sem.at[1, ep],
            {"ep": q * 2 + cc},
        )

    def arrive(q, k):
        z_copy(q, k, 1).wait_recv()

        @pl.when((q < z) & (z + 1 < nz))
        def _():
            z_copy(q, k, 1).start()

        @pl.when((q > z) & (z > 0))
        def _():
            z_copy(q, k, 0).start()

    def make_picks(q, named):
        lane = lax.broadcasted_iota(jnp.int32, (8, rows), 0)
        which = z * 2 + jnp.where(lane == 0, c, 1 - c)
        mask = jnp.where((named[0:1] == which) | (named[1:2] == which), 1.0, 0.0)
        before = jnp.where(
            lax.broadcasted_iota(jnp.int32, (rows, rows), 0)
            < lax.broadcasted_iota(jnp.int32, (rows, rows), 1),
            1.0,
            0.0,
        ).astype(BF16)
        rank = jnp.dot(mask.astype(BF16), before, preferred_element_type=F32)
        key = jnp.where(mask > 0.5, rank, -1.0)
        seat = lax.broadcasted_iota(jnp.int32, (cap, rows), 0).astype(F32)
        for k in range(2):
            picks[q, k * cap : (k + 1) * cap] = jnp.where(
                seat == key[k : k + 1], 1.0, 0.0
            ).astype(BF16)

    def pick_own():
        for k in range(4):
            at = pl.ds(k * share, share)
            got = jnp.dot(picks[z], nrm[:, at], preferred_element_type=F32).astype(BF16)
            xs[z, pl.ds(pl.multiple_of(c * cap, cap), cap), at] = got[:cap]
            own_stage[:, at] = got[cap:]
        own_copy(c).start()

    def pick(q, k):
        got = jnp.dot(picks[q], tok[q, k], preferred_element_type=F32).astype(BF16)
        xs[q, pl.ds(pl.multiple_of(c * cap, cap), cap), columns((t, dg)[k])] = got[:cap]
        stage[q, k] = got[cap:]
        for kind in (range(5), (5,))[k]:
            x_copy(q, kind).start()

    def gate_up(q):
        tile = 256

        @pl.loop(0, gw.shape[1] // tile)
        def _(j):
            cols = pl.ds(pl.multiple_of(j * tile, tile), tile)
            g = jnp.dot(xs[q], gw[:, cols], preferred_element_type=F32)
            u = jnp.dot(xs[q], uw[:, cols], preferred_element_type=F32)
            hid[q, :, cols] = (jax.nn.silu(g) * u).astype(BF16)

    def gathered(q):
        for kind in range(6):
            x_wait(q, kind)

    def ag_start(q):
        for cc in range(2):
            ag_copy(q, cc).start()

    def down(q):
        tile = 256
        for cc in range(2):
            at = pl.ds(cc * cap, cap)
            ag_copy(q, cc).wait_recv()

            @pl.loop(0, span // tile)
            def _(j):
                cols = pl.ds(pl.multiple_of(j * tile, tile), tile)
                psend[q, at, cols] = jnp.dot(
                    hid[q, at], w2[1, :, cols], preferred_element_type=F32
                ).astype(BF16)

            rs_copy(q, cc).start()

        @pl.loop(0, span // tile)
        def _(j):
            cols = pl.ds(pl.multiple_of(j * tile, tile), tile)
            pown[q, :, cols] = jnp.dot(hid[q], w2[0, :, cols], preferred_element_type=F32)

    def give(q):
        for cc in range(2):
            at = pl.ds(cc * cap, cap)
            rs_copy(q, cc).wait_recv()
            res[q, at] = (pown[q, at] + precv[q, at].astype(F32)).astype(BF16)
            ret_copy(q, cc).start()

    def give_own():
        for cc in range(2):
            at = pl.ds(cc * cap, cap)
            rs_copy(z, cc).wait_recv()
            res[z, at] = (pown[z, at] + precv[z, at].astype(F32)).astype(BF16)

            @pl.when(c != cc)
            def _():
                ret_copy(z, cc).start()

    pad = xb.shape[0] - rows

    def halo_copy():
        return remote(
            xb.at[pl.ds(rows, pad)],
            xb.at[pl.ds(0, pad)],
            halo_sem.at[0],
            halo_sem.at[1],
            {"ep": ep + 1},
        )

    def ends_copy(by):
        return remote(
            ends.at[ep],
            ends.at[ep],
            ends_sem.at[0, by],
            ends_sem.at[1, ep],
            {"ep": (ep + by) % n_ep},
        )

    def norm(buffer, gain):
        strip = 64

        @pl.loop(0, rows // strip)
        def _(i):
            at = pl.ds(pl.multiple_of(i * strip, strip), strip)
            wide = buffer[at, :].astype(F32)
            scale = lax.rsqrt(jnp.mean(wide * wide, axis=-1, keepdims=True) + epsilon)
            buffer[at, :] = (wide * scale * gain[...]).astype(BF16)

    def project():
        for k in range(3, 6):
            loads[k].wait()
        norm(mixv, mix_gain_ref)
        tile = 256

        @pl.loop(0, wx.shape[1] // tile)
        def _(j):
            cols = pl.ds(pl.multiple_of(j * tile, tile), tile)
            xb[pl.ds(pad, rows), cols] = jnp.dot(
                mixv[...], wx[:, cols], preferred_element_type=F32
            ).astype(BF16)
            yb[:, cols] = jnp.dot(mixv[...], wy[:, cols], preferred_element_type=F32).astype(BF16)

        @pl.when(ep + 1 < n_ep)
        def _():
            halo_copy().start()

        @pl.when(ep == 0)
        def _():
            xb[pl.ds(0, pad), :] = jnp.zeros((pad, xb.shape[1]), BF16)

    def drives_ready():
        for k in range(6, 9):
            loads[k].wait()

        @pl.when(ep > 0)
        def _():
            halo_copy().wait_recv()

    def drives(heads):
        taps = taps_ref.shape[0]
        size = gaw.shape[1]
        for h in heads:
            cols = pl.ds(h * size, size)
            wide = xb[:, cols].astype(F32)
            conv = jnp.zeros((rows, size), F32)
            for k in range(taps):
                first_row = pad - (taps - 1) + k
                conv = conv + taps_ref[k : k + 1, cols] * wide[first_row : first_row + rows]
            x_conv = conv.astype(BF16)
            gate_a = jnp.dot(x_conv, gaw[h], preferred_element_type=F32)
            gate_x = jnp.dot(x_conv, gxw[h], preferred_element_type=F32)
            log_decay = (
                -lru_scale * jax.nn.sigmoid(gate_a) * soft_plus(-logit_ref[:, cols])
                + shiftv[:, cols]
            )
            av[:, cols] = jnp.exp(log_decay)
            bv[:, cols] = (
                jnp.sqrt(one_minus_exp(2.0 * log_decay))
                * jax.nn.sigmoid(gate_x)
                * x_conv.astype(F32)
            )

    def recur():
        width = av.shape[1]
        row = lax.broadcasted_iota(jnp.int32, (8, width), 0)

        def group(i, carry):
            at = pl.ds(pl.multiple_of(i * 8, 8), 8)
            a, b = av[at, :], bv[at, :]
            for by in (1, 2, 4):
                a_past, b_past = pltpu.roll(a, by, 0), pltpu.roll(b, by, 0)
                b = jnp.where(row >= by, a * b_past + b, b)
                a = jnp.where(row >= by, a * a_past, a)
            b = a * carry[1] + b
            a = a * carry[0]
            av[at, :] = a
            bv[at, :] = b
            return (a[7:8], b[7:8])

        through, state = lax.fori_loop(
            0, rows // 8, group, (jnp.ones((1, width), F32), jnp.zeros((1, width), F32))
        )
        ends[ep, 0:1] = through
        ends[ep, 1:2] = state
        for by in range(1, n_ep):
            ends_copy(by).start()

    def finish():
        carried = jnp.zeros((1, av.shape[1]), F32)
        for by in range(1, n_ep):
            peer = (ep + by) % n_ep
            remote(
                ends.at[peer], ends.at[peer], ends_sem.at[0, 0], ends_sem.at[1, peer], {"ep": peer}
            ).wait_recv()
        for k in range(n_ep):
            entered = ends[k, 0:1] * carried + ends[k, 1:2]
            carried = jnp.where(k < ep, entered, carried)
        strip = 32

        @pl.loop(0, rows // strip)
        def _(i):
            at = pl.ds(pl.multiple_of(i * strip, strip), strip)
            state = bv[at, :] + av[at, :] * carried
            mix_ref[at, :] = (state * jax.nn.gelu(yb[at, :].astype(F32))).astype(BF16)

    def make_combine():
        weights = rw_row[...]
        sides = jnp.concatenate(
            [
                rt_row[...].astype(F32),
                weights / (weights[0:1] + weights[1:2]),
                jnp.zeros((124, rows), F32),
            ],
            axis=0,
        ).T
        one, two = sides[:, 0:1].astype(jnp.int32), sides[:, 1:2].astype(jnp.int32)
        lane = lax.broadcasted_iota(jnp.int32, (rows, 128), 1)
        mask = jnp.where((one == lane) | (two == lane), 1.0, 0.0)
        before = jnp.where(
            lax.broadcasted_iota(jnp.int32, (rows, rows), 1)
            < lax.broadcasted_iota(jnp.int32, (rows, rows), 0),
            1.0,
            0.0,
        ).astype(BF16)
        rank = jnp.dot(before, mask.astype(BF16), preferred_element_type=F32)
        key = jnp.where(mask > 0.5, rank, -1.0)
        part_one, part_two = sides[:, 2:3], sides[:, 3:4]
        seat = lax.broadcasted_iota(jnp.int32, (rows, cap), 1).astype(F32)
        for e in range(n_ep):
            comb[e] = jnp.where(seat == key[:, e : e + 1], 1.0, 0.0).astype(BF16)
            part[e] = jnp.broadcast_to(
                jnp.where(one == e, part_one, 0.0) + jnp.where(two == e, part_two, 0.0),
                (rows, 128),
            )

    def combine(e, rows_in, first=False, last=False):
        got = jnp.dot(comb[e], rows_in, preferred_element_type=F32)
        for j in range(got.shape[1] // 128):
            at = pl.ds(j * 128, 128)
            term = part[e] * got[:, j * 128 : (j + 1) * 128]
            if not first:
                term = total[:, at] + term
            if last:
                out_ref[:, at] = term.astype(BF16)
            else:
                total[:, at] = term

    def ret_wait(e):
        remote(
            res.at[0, pl.ds(0, cap)], ret.at[e], ret_sem.at[0, 0], ret_sem.at[1, e], {"ep": other}
        ).wait_recv()

    def combine_plane(q, first=False, last=False):
        for cc in range(2):
            ret_wait(q * 2 + cc)
            combine(q * 2 + cc, ret[q * 2 + cc], first and cc == 0, last and cc == 1)

    loads[0].wait()
    norm(nrm, gain_ref)
    pl.semaphore_wait(barrier, n_ep + 3)
    for q in range(nz):

        @pl.when(q != z)
        def _():
            route_copy(q).start()

    for k in range(2):

        @pl.when(z + 1 < nz)
        def _():
            z_own(k, 1).start()

        @pl.when(z > 0)
        def _():
            z_own(k, 0).start()

    for k in range(3):
        w_copy(k).start()
    make_picks(z, rt_row[...])
    pick_own()
    project()
    one, two, three = block_at(0), block_at(1), block_at(2)
    for q in (one, two, three):
        remote(
            rt_row, routes_all.at[q], rt_sem.at[0, 0], rt_sem.at[1, q], {"ep": q * 2 + c}
        ).wait_recv()
        make_picks(q, routes_all[q])
    own_copy(1 - c).wait_recv()
    for k in range(1, 3):
        loads[k].wait()
    gate_up(z)
    arrive(one, 0)
    pick(one, 0)
    w_copy(3).start()

    @pl.when(inner)
    def _():
        arrive(three, 0)

    drives_ready()
    drives(range(0, 4))
    make_combine()
    arrive(one, 1)
    pick(one, 1)

    @pl.when(inner)
    def _():
        arrive(three, 1)

    recur()
    gathered(one)
    gate_up(one)
    ag_start(one)
    arrive(two, 0)
    pick(two, 0)
    for k in range(9, 11):
        loads[k].wait()
    for k in range(4):
        w_copy(k).wait_recv()
    down(one)
    arrive(two, 1)
    pick(two, 1)
    gathered(two)
    gate_up(two)
    ag_start(two)
    give(one)

    @pl.when(jnp.logical_not(inner))
    def _():
        arrive(three, 0)

    pick(three, 0)
    down(two)
    finish()

    @pl.when(jnp.logical_not(inner))
    def _():
        arrive(three, 1)

    pick(three, 1)
    give(two)
    gathered(three)
    gate_up(three)
    ag_start(three)
    combine_plane(one, first=True)
    down(three)
    ag_start(z)
    give(three)
    down(z)
    combine_plane(two)
    give_own()
    combine(ep, res[z, pl.ds(pl.multiple_of(c * cap, cap), cap)])
    ret_wait(other)
    combine(other, ret[other])
    combine_plane(three, last=True)

    for k in range(2):

        @pl.when(z + 1 < nz)
        def _():
            z_own(k, 1).wait_send()

        @pl.when(z > 0)
        def _():
            z_own(k, 0).wait_send()

    for k in range(4):
        w_copy(k).wait_send()

    own_copy(c).wait_send()

    @pl.when(ep + 1 < n_ep)
    def _():
        halo_copy().wait_send()

    for by in range(1, n_ep):
        ends_copy(by).wait_send()

    def drain(q, carry):
        for cc in range(2):
            ag_copy(q, cc).wait_send()
            rs_copy(q, cc).wait_send()

        @pl.when(q != z)
        def _():
            route_copy(q).wait_send()
            for kind in range(6):
                x_copy(q, kind).wait_send()

        for k in range(2):

            @pl.when((q < z) & (z + 1 < nz))
            def _():
                z_copy(q, k, 1).wait_send()

            @pl.when((q > z) & (z > 0))
            def _():
                z_copy(q, k, 0).wait_send()

        for cc in range(2):

            @pl.when((q != z) | (c != cc))
            def _():
                ret_copy(q, cc).wait_send()

        return carry

    lax.fori_loop(0, nz, drain, 0)


def both_fused(
    mix_in,
    mix_gain,
    w_in_x,
    w_in_y,
    conv_taps,
    recur_gate_w,
    input_gate_w,
    decay_logit,
    decay_shift,
    moe_in,
    moe_gain,
    routes,
    route_weight,
    expert_gate,
    expert_up,
    expert_down,
):
    n_ep = lax.axis_size("ep")
    nz = n_ep // 2
    rows, features = moe_in.shape
    share = features // 4
    ff_dev, out_dev = expert_gate.shape[2], expert_down.shape[2]
    width = w_in_x.shape[1]
    cap = 2 * rows * routes.shape[1] // n_ep
    pair = 2 * cap
    vmem = pl.BlockSpec(memory_space=pltpu.VMEM)
    hbm = pl.BlockSpec(memory_space=pltpu.HBM)
    dma = pltpu.SemaphoreType.DMA
    flops = 2 * n_ep * cap * features * (2 * ff_dev + out_dev)
    return pl.pallas_call(
        functools.partial(both_kernel, cap),
        out_shape=(
            jax.ShapeDtypeStruct((rows, width), BF16),
            jax.ShapeDtypeStruct((rows, out_dev), BF16),
        ),
        in_specs=[hbm] * 6 + [vmem] * 3 + [hbm] + [vmem] * 3 + [hbm] * 3,
        out_specs=(vmem, vmem),
        scratch_shapes=[
            pltpu.VMEM((rows, features), BF16),
            pltpu.VMEM((nz, 2, rows, share), BF16),
            pltpu.VMEM((nz, pair, features), BF16),
            pltpu.VMEM((nz, 2, cap, share), BF16),
            pltpu.VMEM((cap, features), BF16),
            pltpu.VMEM((nz, pair, rows), BF16),
            pltpu.VMEM((nz, pair, 2 * ff_dev), BF16),
            pltpu.VMEM((nz, pair, out_dev), BF16),
            pltpu.VMEM((nz, pair, out_dev), BF16),
            pltpu.VMEM((nz, pair, out_dev), F32),
            pltpu.VMEM((nz, pair, out_dev), BF16),
            pltpu.VMEM((n_ep, cap, out_dev), BF16),
            pltpu.VMEM((nz, 2, rows), jnp.int32),
            pltpu.VMEM((n_ep, rows, cap), BF16),
            pltpu.VMEM((n_ep, rows, 128), F32),
            pltpu.VMEM((rows, out_dev), F32),
            pltpu.VMEM(expert_gate.shape[1:], BF16),
            pltpu.VMEM(expert_up.shape[1:], BF16),
            pltpu.VMEM((2, 2 * ff_dev, out_dev), BF16),
            dma((11,)),
            dma((2, nz)),
            dma((2, 2, nz)),
            dma((2, nz)),
            dma((2, 4)),
            dma((6, nz)),
            dma((6, nz)),
            dma((2, n_ep)),
            dma((2, n_ep)),
            dma((2, n_ep)),
            pltpu.VMEM(mix_in.shape, BF16),
            pltpu.VMEM(w_in_x.shape, BF16),
            pltpu.VMEM(w_in_y.shape, BF16),
            pltpu.VMEM(recur_gate_w.shape, BF16),
            pltpu.VMEM(input_gate_w.shape, BF16),
            pltpu.VMEM((rows, width), F32),
            pltpu.VMEM((16 + rows, width), BF16),
            pltpu.VMEM((rows, width), BF16),
            pltpu.VMEM((rows, width), F32),
            pltpu.VMEM((rows, width), F32),
            pltpu.VMEM((n_ep, 2, width), F32),
            dma((2,)),
            dma((2, n_ep)),
        ],
        compiler_params=pltpu.CompilerParams(
            collective_id=0, has_side_effects=True, vmem_limit_bytes=60 * 1024 * 1024
        ),
        cost_estimate=pl.CostEstimate(flops=flops, bytes_accessed=16 << 20, transcendentals=0),
        name="both",
    )(
        mix_in,
        w_in_x,
        w_in_y,
        recur_gate_w,
        input_gate_w,
        decay_shift,
        mix_gain[None, :],
        conv_taps,
        decay_logit[None, :],
        moe_in,
        moe_gain[None, :],
        routes.T,
        route_weight.T,
        expert_gate,
        expert_up,
        expert_down,
    )


def from_behind(value, axis, by):
    count = lax.axis_size(axis)
    pairs = [(i, i + by) for i in range(count) if 0 <= i + by < count]
    return lax.ppermute(value, axis, pairs)


def entering(value, axis, combine, identity):
    count, index = (lax.axis_size(axis), lax.axis_index(axis))
    everything = jax.tree.map(lambda part: lax.all_gather(part, axis), value)
    start = jax.tree.map(
        lambda part, zero: jnp.broadcast_to(jnp.asarray(zero, part.dtype), part.shape),
        value,
        identity,
    )

    def hop(k, before):
        reached = k < index
        new = combine(before, jax.tree.map(lambda part: part[k], everything))
        return jax.tree.map(lambda a, b: jnp.where(reached, a, b), new, before)

    return lax.fori_loop(0, count, hop, start)


def norm_rows(rows, gain):
    widened = rows.astype(jnp.float32)
    scaled = widened * lax.rsqrt(jnp.mean(widened * widened, axis=-1, keepdims=True) + epsilon)
    return (scaled * gain[None, :]).astype(jnp.bfloat16)


def link(earlier, later):
    return (earlier[0] * later[0], later[0] * earlier[1] + later[1])


def fits_fused(moe_in, routes):
    n_ep = lax.axis_size("ep")
    gathered = n_ep * moe_in.size * moe_in.dtype.itemsize
    even = n_ep == 4 * routes.shape[1] == 2 * len(block_order)
    return lax.axis_size("tp") == 4 and even and gathered <= (16 << 20)


def moe_staged(moe_in, moe_gain, routes, route_weight, expert_gate, expert_up, expert_down):
    moe_rows = norm_rows(moe_in, moe_gain)
    token_count = moe_rows.shape[0]
    feature_count = moe_rows.shape[1]
    choose_count = routes.shape[1]
    expert_count = lax.axis_size("ep")
    capacity = 2 * token_count * choose_count // expert_count
    slot_total = expert_count * capacity
    expert_ids = routes.reshape(-1)
    onehot = (expert_ids[:, None] == jnp.arange(expert_count, dtype=jnp.int32)[None, :]).astype(
        jnp.int32
    )
    slot_rank = jnp.sum(jnp.cumsum(onehot, axis=0) * onehot, axis=1) - 1
    slot_index = expert_ids * capacity + slot_rank
    token_index = jnp.repeat(jnp.arange(token_count, dtype=jnp.int32), choose_count)
    slot_owner = jnp.full((slot_total,), token_count, jnp.int32).at[slot_index].set(token_index)
    padded_rows = jnp.concatenate([moe_rows, jnp.zeros((1, feature_count), jnp.bfloat16)], axis=0)
    outgoing = padded_rows[slot_owner].reshape(expert_count, capacity, feature_count)
    column_width = feature_count // lax.axis_size("tp")
    own_columns = lax.dynamic_slice_in_dim(
        outgoing, lax.axis_index("tp") * column_width, column_width, 2
    )
    incoming = lax.all_to_all(own_columns, "ep", split_axis=0, concat_axis=0, tiled=True)
    piece = lax.all_gather(incoming, "tp", axis=2, tiled=True)
    flat_rows = piece.reshape(slot_total, piece.shape[2])
    gate_rows = expert_gate[0]
    up_rows = expert_up[0]
    gate_proj = jnp.dot(flat_rows, gate_rows, preferred_element_type=jnp.float32)
    up_proj = jnp.dot(flat_rows, up_rows, preferred_element_type=jnp.float32)
    hidden = (jax.nn.silu(gate_proj) * up_proj).astype(jnp.bfloat16)
    down_rows = expert_down[0]
    columns = jnp.dot(
        lax.all_gather(hidden, "tp", axis=1, tiled=True),
        down_rows,
        preferred_element_type=jnp.float32,
    )
    results = columns.astype(jnp.bfloat16).reshape(expert_count, capacity, expert_down.shape[2])
    returned = lax.all_to_all(results, "ep", split_axis=0, concat_axis=0, tiled=True).reshape(
        slot_total, expert_down.shape[2]
    )
    picked = (
        returned[slot_index]
        .astype(jnp.float32)
        .reshape(token_count, choose_count, expert_down.shape[2])
    )
    route_share = route_weight / jnp.sum(route_weight, axis=1, keepdims=True)
    moe_out = jnp.sum(route_share[:, :, None] * picked, axis=1).astype(jnp.bfloat16)
    return moe_out


def staged(
    mix_in,
    mix_gain,
    w_in_x,
    w_in_y,
    conv_taps,
    recur_gate_w,
    input_gate_w,
    decay_logit,
    decay_shift,
    moe_in,
    moe_gain,
    routes,
    route_weight,
    expert_gate,
    expert_up,
    expert_down,
):
    row_count = mix_in.shape[0]
    width_dev = w_in_x.shape[1]
    heads_dev = recur_gate_w.shape[0]
    block_size = recur_gate_w.shape[1]
    tap_count = conv_taps.shape[0]
    mixer_rows = norm_rows(mix_in, mix_gain)
    x_branch = jnp.dot(mixer_rows, w_in_x, preferred_element_type=jnp.float32).astype(jnp.bfloat16)
    y_branch = jnp.dot(mixer_rows, w_in_y, preferred_element_type=jnp.float32).astype(jnp.bfloat16)
    previous = from_behind(x_branch[row_count - (tap_count - 1) :], "ep", 1)
    padded = jnp.concatenate([previous, x_branch], axis=0)
    conv_sum = jnp.zeros((row_count, width_dev), jnp.float32)
    for tap_index in range(tap_count):
        conv_sum = conv_sum + conv_taps[tap_index][None, :] * padded[
            tap_index : tap_index + row_count
        ].astype(jnp.float32)
    x_conv = conv_sum.astype(jnp.bfloat16)
    heads_in = x_conv.reshape(row_count, heads_dev, block_size)
    gate_a = jnp.einsum(
        "thi,hij->thj", heads_in, recur_gate_w, preferred_element_type=jnp.float32
    ).reshape(row_count, width_dev)
    gate_x = jnp.einsum(
        "thi,hij->thj", heads_in, input_gate_w, preferred_element_type=jnp.float32
    ).reshape(row_count, width_dev)
    log_decay = (
        -lru_scale * jax.nn.sigmoid(gate_a) * jax.nn.softplus(-decay_logit)[None, :] + decay_shift
    )
    lru_drive = (
        jnp.sqrt(-jnp.expm1(2.0 * log_decay)) * jax.nn.sigmoid(gate_x) * x_conv.astype(jnp.float32)
    )
    through, local_state = lax.associative_scan(link, (jnp.exp(log_decay), lru_drive), axis=0)
    identity = (jnp.ones((width_dev,), jnp.float32), jnp.zeros((width_dev,), jnp.float32))
    carried = entering((through[row_count - 1], local_state[row_count - 1]), "ep", link, identity)
    lru_state = local_state + through * carried[1][None, :]
    mixer_out = (lru_state * jax.nn.gelu(y_branch.astype(jnp.float32))).astype(jnp.bfloat16)
    moe_out = moe_staged(
        moe_in, moe_gain, routes, route_weight, expert_gate, expert_up, expert_down
    )
    return (mixer_out, moe_out)


def local(*args):
    return (both_fused if fits_fused(args[9], args[11]) else staged)(*args)


def solution(mesh):
    placed = (
        P("ep", None),
        P(),
        P(None, "tp"),
        P(None, "tp"),
        P(None, "tp"),
        P("tp", None, None),
        P("tp", None, None),
        P("tp"),
        P("ep", "tp"),
        P("ep", None),
        P(),
        P("ep", None),
        P("ep", None),
        P("ep", None, "tp"),
        P("ep", None, "tp"),
        P("ep", None, "tp"),
    )
    return jax.shard_map(
        local, mesh=mesh, in_specs=placed, out_specs=(P("ep", "tp"), P("ep", "tp")), check_vma=False
    )
```

```python
import functools

import jax
import jax.numpy as jnp
from jax import lax
from jax.experimental import pallas as pl
from jax.experimental.pallas import tpu as pltpu
from jax.sharding import PartitionSpec as P

epsilon = 1e-06
lru_scale = 8.0
MESH = pl.DeviceIdType.MESH
F32 = jnp.float32
BF16 = jnp.bfloat16


block_order = ((1, 2, 3), (2, 3, 0), (1, 0, 3), (2, 1, 0))


def one_minus_exp(value):
    series = jnp.full_like(value, 1.0 / 9.0)
    for k in range(8, 1, -1):
        series = (1.0 + value * series) * (1.0 / k)
    series = 1.0 + value * series
    return jnp.where(value > -0.5, -value * series, 1.0 - jnp.exp(value))


def soft_plus(value):
    small = jnp.exp(-jnp.abs(value))
    series = jnp.full_like(small, 1.0 / 7.0)
    for k in range(6, 0, -1):
        series = 1.0 / k - small * series
    wide = jnp.where(small < 0.05, small * series, jnp.log(1.0 + small))
    return jnp.maximum(value, 0.0) + wide


def both_kernel(
    cap,
    mix_hbm,
    wx_hbm,
    wy_hbm,
    ga_hbm,
    gx_hbm,
    shift_hbm,
    mix_gain_ref,
    taps_ref,
    logit_ref,
    moe_hbm,
    gain_ref,
    rt_row,
    rw_row,
    gate_hbm,
    up_hbm,
    down_hbm,
    mix_ref,
    out_ref,
    nrm,
    tok,
    xs,
    stage,
    own_stage,
    picks,
    hid,
    psend,
    precv,
    pown,
    res,
    ret,
    routes_all,
    comb,
    part,
    total,
    gw,
    uw,
    w2,
    load_sem,
    rt_sem,
    z_send,
    z_recv,
    w_sem,
    x_send,
    x_recv,
    ag_sem,
    rs_sem,
    ret_sem,
    mixv,
    wx,
    wy,
    gaw,
    gxw,
    shiftv,
    xb,
    yb,
    av,
    bv,
    ends,
    halo_sem,
    ends_sem,
):
    n_ep = lax.axis_size("ep")
    nz = n_ep // 2
    ep = lax.axis_index("ep")
    t = lax.axis_index("tp")
    z, c = ep // 2, ep % 2
    y, x = t // 2, t % 2
    xp, yp, dg = y * 2 + (1 - x), (1 - y) * 2 + x, 3 - t
    pa, pb = jnp.where(c == 0, xp, yp), jnp.where(c == 0, yp, xp)
    other = z * 2 + (1 - c)
    rows, share = tok.shape[2], tok.shape[3]
    inner = (z > 0) & (z + 1 < nz)
    outer = jnp.logical_not(inner)
    shares = (t, dg, xp, yp)

    def block_at(s):
        q = jnp.int32(0)
        for zz in range(nz):
            q = jnp.where(z == zz, block_order[zz][s], q)
        return q

    def remote(src, dst, send, recv, where):
        return pltpu.make_async_remote_copy(
            src_ref=src,
            dst_ref=dst,
            send_sem=send,
            recv_sem=recv,
            device_id=where,
            device_id_type=MESH,
        )

    span = w2.shape[2]
    half = w2.shape[1] // 2

    def down_rows(k):
        return down_hbm.at[0, pl.ds(pl.multiple_of(k * half, half), half)]

    loads = [
        pltpu.make_async_copy(moe_hbm, nrm, load_sem.at[0]),
        pltpu.make_async_copy(gate_hbm.at[0], gw, load_sem.at[1]),
        pltpu.make_async_copy(up_hbm.at[0], uw, load_sem.at[2]),
        pltpu.make_async_copy(mix_hbm, mixv, load_sem.at[3]),
        pltpu.make_async_copy(wx_hbm, wx, load_sem.at[4]),
        pltpu.make_async_copy(wy_hbm, wy, load_sem.at[5]),
        pltpu.make_async_copy(ga_hbm, gaw, load_sem.at[6]),
        pltpu.make_async_copy(gx_hbm, gxw, load_sem.at[7]),
        pltpu.make_async_copy(shift_hbm, shiftv, load_sem.at[8]),
        pltpu.make_async_copy(down_rows(t), w2.at[0, pl.ds(0, half)], load_sem.at[9]),
        pltpu.make_async_copy(down_rows(pa), w2.at[0, pl.ds(half, half)], load_sem.at[10]),
    ]
    loads[0].start()
    barrier = pltpu.get_barrier_semaphore()
    for by in range(1, n_ep):
        pl.semaphore_signal(
            barrier, inc=1, device_id={"ep": (ep + by) % n_ep}, device_id_type=MESH
        )
    for peer in (xp, yp):
        for near in (ep, other):
            pl.semaphore_signal(
                barrier, inc=1, device_id={"ep": near, "tp": peer}, device_id_type=MESH
            )
    for copy in loads[3:6] + loads[1:3] + loads[6:]:
        copy.start()

    def columns(k):
        return pl.ds(pl.multiple_of(k * share, share), share)

    def z_own(k, up):
        return remote(
            nrm.at[:, columns(shares[k])],
            tok.at[z, k],
            z_send.at[up, k, z],
            z_recv.at[k, z],
            {"ep": ep + (2 if up else -2)},
        )

    def z_copy(q, k, up):
        return remote(
            tok.at[q, k],
            tok.at[q, k],
            z_send.at[up, k, q],
            z_recv.at[k, q],
            {"ep": ep + (2 if up else -2)},
        )

    def route_copy(q):
        return remote(rt_row, routes_all.at[z], rt_sem.at[0, q], rt_sem.at[1, z], {"ep": q * 2 + c})

    def w_copy(k):
        piece = half // 2
        first = (pb, dg)[k // 2] * half + k % 2 * piece
        return remote(
            down_hbm.at[0, pl.ds(pl.multiple_of(first, piece), piece)],
            w2.at[1, pl.ds(k * piece, piece)],
            w_sem.at[0, k],
            w_sem.at[1, k],
            {"tp": pb},
        )

    def xs_part(q, block, k):
        return xs.at[q, pl.ds(pl.multiple_of(block * cap, cap), cap), columns(k)]

    def x_copy(q, kind):
        to = (xp, yp, xp, yp, t, t, t, t)[kind]
        near = ep if kind < 2 else other
        src = xs_part(q, c, t) if kind < 2 else stage.at[q, max(kind - 4, 0)]
        return remote(
            src,
            xs_part(q, c, shares[max(kind - 4, 0)]),
            x_send.at[kind, q],
            x_recv.at[kind, q],
            {"ep": near, "tp": to},
        )

    def x_wait(q, kind):
        block = c if kind < 2 else 1 - c
        dst = xs_part(q, block, (xp, yp, xp, yp, t, dg, xp, yp)[kind])
        remote(
            stage.at[q, 0], dst, x_send.at[kind, q], x_recv.at[kind, q], {"ep": other}
        ).wait_recv()

    def own_copy(block):
        return remote(
            own_stage,
            xs.at[z, pl.ds(pl.multiple_of(block * cap, cap), cap)],
            x_send.at[4, z],
            x_recv.at[4, z],
            {"ep": other},
        )

    def ag_copy(q, cc):
        at, sem = pl.ds(cc * cap, cap), q * 2 + cc
        return remote(
            hid.at[q, at, pl.ds(0, half)],
            hid.at[q, at, pl.ds(half, half)],
            ag_sem.at[0, sem],
            ag_sem.at[1, sem],
            {"tp": pa},
        )

    def rs_copy(q, cc):
        at, sem = pl.ds(cc * cap, cap), q * 2 + cc
        return remote(
            psend.at[q, at], precv.at[q, at], rs_sem.at[0, sem], rs_sem.at[1, sem], {"tp": pb}
        )

    def ret_copy(q, cc):
        return remote(
            res.at[q, pl.ds(cc * cap, cap)],
            ret.at[ep],
            ret_sem.at[0, q * 2 + cc],
            ret_sem.at[1, ep],
            {"ep": q * 2 + cc},
        )

    def arrive(q, k):
        z_copy(q, k, 1).wait_recv()
        if k < 2:

            @pl.when((q < z) & (z + 1 < nz))
            def _():
                z_copy(q, k, 1).start()

            @pl.when((q > z) & (z > 0))
            def _():
                z_copy(q, k, 0).start()

    def make_picks(q, named):
        lane = lax.broadcasted_iota(jnp.int32, (8, rows), 0)
        which = z * 2 + jnp.where(lane == 0, c, 1 - c)
        mask = jnp.where((named[0:1] == which) | (named[1:2] == which), 1.0, 0.0)
        before = jnp.where(
            lax.broadcasted_iota(jnp.int32, (rows, rows), 0)
            < lax.broadcasted_iota(jnp.int32, (rows, rows), 1),
            1.0,
            0.0,
        ).astype(BF16)
        rank = jnp.dot(mask.astype(BF16), before, preferred_element_type=F32)
        key = jnp.where(mask > 0.5, rank, -1.0)
        seat = lax.broadcasted_iota(jnp.int32, (cap, rows), 0).astype(F32)
        for k in range(2):
            picks[q, k * cap : (k + 1) * cap] = jnp.where(
                seat == key[k : k + 1], 1.0, 0.0
            ).astype(BF16)

    def pick_own():
        for k in range(4):
            at = pl.ds(k * share, share)
            got = jnp.dot(picks[z], nrm[:, at], preferred_element_type=F32).astype(BF16)
            xs[z, pl.ds(pl.multiple_of(c * cap, cap), cap), at] = got[:cap]
            own_stage[:, at] = got[cap:]
        own_copy(c).start()

    def pick(q, k, whole=False):
        got = jnp.dot(picks[q], tok[q, k], preferred_element_type=F32).astype(BF16)
        xs[q, pl.ds(pl.multiple_of(c * cap, cap), cap), columns(shares[k])] = got[:cap]
        stage[q, k] = got[cap:]
        for kind in range(5) if k == 0 and not whole else (4 + k,):
            x_copy(q, kind).start()

    def gate_up(q):
        tile = 256

        @pl.loop(0, gw.shape[1] // tile)
        def _(j):
            cols = pl.ds(pl.multiple_of(j * tile, tile), tile)
            g = jnp.dot(xs[q], gw[:, cols], preferred_element_type=F32)
            u = jnp.dot(xs[q], uw[:, cols], preferred_element_type=F32)
            hid[q, :, cols] = (jax.nn.silu(g) * u).astype(BF16)

    def gathered(q, kinds=range(6)):
        for kind in kinds:
            x_wait(q, kind)

    def ag_start(q):
        for cc in range(2):
            ag_copy(q, cc).start()

    def down_other(q, cc):
        tile = 256
        at = pl.ds(cc * cap, cap)
        ag_copy(q, cc).wait_recv()

        @pl.loop(0, span // tile)
        def _(j):
            cols = pl.ds(pl.multiple_of(j * tile, tile), tile)
            psend[q, at, cols] = jnp.dot(
                hid[q, at], w2[1, :, cols], preferred_element_type=F32
            ).astype(BF16)

        rs_copy(q, cc).start()

    def down_own(q):
        tile = 256

        @pl.loop(0, span // tile)
        def _(j):
            cols = pl.ds(pl.multiple_of(j * tile, tile), tile)
            pown[q, :, cols] = jnp.dot(hid[q], w2[0, :, cols], preferred_element_type=F32)

    def give(q, cc):
        at = pl.ds(cc * cap, cap)
        rs_copy(q, cc).wait_recv()
        res[q, at] = (pown[q, at] + precv[q, at].astype(F32)).astype(BF16)
        ret_copy(q, cc).start()

    def give_own():
        for cc in range(2):
            at = pl.ds(cc * cap, cap)
            rs_copy(z, cc).wait_recv()
            res[z, at] = (pown[z, at] + precv[z, at].astype(F32)).astype(BF16)

            @pl.when(c != cc)
            def _():
                ret_copy(z, cc).start()

    pad = xb.shape[0] - rows

    def halo_copy():
        return remote(
            xb.at[pl.ds(rows, pad)],
            xb.at[pl.ds(0, pad)],
            halo_sem.at[0],
            halo_sem.at[1],
            {"ep": ep + 1},
        )

    def ends_copy(by):
        return remote(
            ends.at[ep],
            ends.at[ep],
            ends_sem.at[0, by],
            ends_sem.at[1, ep],
            {"ep": (ep + by) % n_ep},
        )

    def norm(buffer, gain):
        strip = 64

        @pl.loop(0, rows // strip)
        def _(i):
            at = pl.ds(pl.multiple_of(i * strip, strip), strip)
            wide = buffer[at, :].astype(F32)
            scale = lax.rsqrt(jnp.mean(wide * wide, axis=-1, keepdims=True) + epsilon)
            buffer[at, :] = (wide * scale * gain[...]).astype(BF16)

    def project():
        for k in range(3, 6):
            loads[k].wait()
        norm(mixv, mix_gain_ref)
        tile = 256

        @pl.loop(0, wx.shape[1] // tile)
        def _(j):
            cols = pl.ds(pl.multiple_of(j * tile, tile), tile)
            xb[pl.ds(pad, rows), cols] = jnp.dot(
                mixv[...], wx[:, cols], preferred_element_type=F32
            ).astype(BF16)
            yb[:, cols] = jnp.dot(mixv[...], wy[:, cols], preferred_element_type=F32).astype(BF16)

        @pl.when(ep + 1 < n_ep)
        def _():
            halo_copy().start()

        @pl.when(ep == 0)
        def _():
            xb[pl.ds(0, pad), :] = jnp.zeros((pad, xb.shape[1]), BF16)

    def drives_ready():
        for k in range(6, 9):
            loads[k].wait()

        @pl.when(ep > 0)
        def _():
            halo_copy().wait_recv()

    def drives(heads):
        taps = taps_ref.shape[0]
        size = gaw.shape[1]
        for h in heads:
            cols = pl.ds(h * size, size)
            wide = xb[:, cols].astype(F32)
            conv = jnp.zeros((rows, size), F32)
            for k in range(taps):
                first_row = pad - (taps - 1) + k
                conv = conv + taps_ref[k : k + 1, cols] * wide[first_row : first_row + rows]
            x_conv = conv.astype(BF16)
            gate_a = jnp.dot(x_conv, gaw[h], preferred_element_type=F32)
            gate_x = jnp.dot(x_conv, gxw[h], preferred_element_type=F32)
            log_decay = (
                -lru_scale * jax.nn.sigmoid(gate_a) * soft_plus(-logit_ref[:, cols])
                + shiftv[:, cols]
            )
            av[:, cols] = jnp.exp(log_decay)
            bv[:, cols] = (
                jnp.sqrt(one_minus_exp(2.0 * log_decay))
                * jax.nn.sigmoid(gate_x)
                * x_conv.astype(F32)
            )

    def recur():
        width = av.shape[1]
        row = lax.broadcasted_iota(jnp.int32, (8, width), 0)

        def group(i, carry):
            at = pl.ds(pl.multiple_of(i * 8, 8), 8)
            a, b = av[at, :], bv[at, :]
            for by in (1, 2, 4):
                a_past, b_past = pltpu.roll(a, by, 0), pltpu.roll(b, by, 0)
                b = jnp.where(row >= by, a * b_past + b, b)
                a = jnp.where(row >= by, a * a_past, a)
            b = a * carry[1] + b
            a = a * carry[0]
            av[at, :] = a
            bv[at, :] = b
            return (a[7:8], b[7:8])

        through, state = lax.fori_loop(
            0, rows // 8, group, (jnp.ones((1, width), F32), jnp.zeros((1, width), F32))
        )
        ends[ep, 0:1] = through
        ends[ep, 1:2] = state
        for by in range(1, n_ep):
            ends_copy(by).start()

    def finish():
        carried = jnp.zeros((1, av.shape[1]), F32)
        for by in range(1, n_ep):
            peer = (ep + by) % n_ep
            remote(
                ends.at[peer], ends.at[peer], ends_sem.at[0, 0], ends_sem.at[1, peer], {"ep": peer}
            ).wait_recv()
        for k in range(n_ep):
            entered = ends[k, 0:1] * carried + ends[k, 1:2]
            carried = jnp.where(k < ep, entered, carried)
        strip = 32

        @pl.loop(0, rows // strip)
        def _(i):
            at = pl.ds(pl.multiple_of(i * strip, strip), strip)
            state = bv[at, :] + av[at, :] * carried
            mix_ref[at, :] = (state * jax.nn.gelu(yb[at, :].astype(F32))).astype(BF16)

    def make_combine():
        weights = rw_row[...]
        sides = jnp.concatenate(
            [
                rt_row[...].astype(F32),
                weights / (weights[0:1] + weights[1:2]),
                jnp.zeros((124, rows), F32),
            ],
            axis=0,
        ).T
        one, two = sides[:, 0:1].astype(jnp.int32), sides[:, 1:2].astype(jnp.int32)
        lane = lax.broadcasted_iota(jnp.int32, (rows, 128), 1)
        mask = jnp.where((one == lane) | (two == lane), 1.0, 0.0)
        before = jnp.where(
            lax.broadcasted_iota(jnp.int32, (rows, rows), 1)
            < lax.broadcasted_iota(jnp.int32, (rows, rows), 0),
            1.0,
            0.0,
        ).astype(BF16)
        rank = jnp.dot(before, mask.astype(BF16), preferred_element_type=F32)
        key = jnp.where(mask > 0.5, rank, -1.0)
        part_one, part_two = sides[:, 2:3], sides[:, 3:4]
        seat = lax.broadcasted_iota(jnp.int32, (rows, cap), 1).astype(F32)
        for e in range(n_ep):
            comb[e] = jnp.where(seat == key[:, e : e + 1], 1.0, 0.0).astype(BF16)
            part[e] = jnp.broadcast_to(
                jnp.where(one == e, part_one, 0.0) + jnp.where(two == e, part_two, 0.0),
                (rows, 128),
            )

    def combine(e, rows_in, first=False, last=False):
        got = jnp.dot(comb[e], rows_in, preferred_element_type=F32)
        for j in range(got.shape[1] // 128):
            at = pl.ds(j * 128, 128)
            term = part[e] * got[:, j * 128 : (j + 1) * 128]
            if not first:
                term = total[:, at] + term
            if last:
                out_ref[:, at] = term.astype(BF16)
            else:
                total[:, at] = term

    def ret_wait(e):
        remote(
            res.at[0, pl.ds(0, cap)], ret.at[e], ret_sem.at[0, 0], ret_sem.at[1, e], {"ep": other}
        ).wait_recv()

    def combine_far(e, first=False, last=False):
        ret_wait(e)
        combine(e, ret[e], first, last)

    loads[0].wait()
    norm(nrm, gain_ref)
    pl.semaphore_wait(barrier, n_ep + 3)
    for q in range(nz):

        @pl.when(q != z)
        def _():
            route_copy(q).start()

    for k in range(4):

        @pl.when((z + 1 < nz) & ((z == 0) | (k < 2)))
        def _():
            z_own(k, 1).start()

        @pl.when((z > 0) & ((z + 1 == nz) | (k < 2)))
        def _():
            z_own(k, 0).start()

    for k in range(3):
        w_copy(k).start()
    make_picks(z, rt_row[...])
    pick_own()
    one, two, three = block_at(0), block_at(1), block_at(2)
    for q in (one, two, three):
        remote(
            rt_row, routes_all.at[q], rt_sem.at[0, 0], rt_sem.at[1, q], {"ep": q * 2 + c}
        ).wait_recv()
        make_picks(q, routes_all[q])
    project()
    own_copy(1 - c).wait_recv()
    for k in range(1, 3):
        loads[k].wait()
    gate_up(z)
    arrive(one, 0)
    pick(one, 0)
    w_copy(3).start()

    @pl.when(inner)
    def _():
        arrive(three, 0)

    make_combine()
    arrive(one, 1)
    pick(one, 1)

    @pl.when(inner)
    def _():
        arrive(three, 1)

    gathered(one)
    gate_up(one)
    ag_start(one)
    arrive(two, 0)
    pick(two, 0)
    for k in range(9, 11):
        loads[k].wait()
    for k in range(4):
        w_copy(k).wait_recv()
    down_other(one, 0)
    down_other(one, 1)
    down_own(one)
    arrive(two, 1)
    pick(two, 1)
    gathered(two)
    gate_up(two)
    ag_start(two)
    drives_ready()
    drives(range(0, 4))
    give(one, 0)
    give(one, 1)
    recur()

    @pl.when(outer)
    def _():
        arrive(three, 0)
        pick(three, 0)

    @pl.when(inner)
    def _():
        pick(three, 0, True)

    down_other(two, 0)
    ag_start(z)
    down_other(two, 1)
    down_own(two)

    @pl.when(outer)
    def _():
        arrive(three, 1)
        pick(three, 1)

    @pl.when(inner)
    def _():
        pick(three, 1)
        for k in range(2, 4):
            arrive(three, k)
            pick(three, k)


    @pl.when(outer)
    def _():
        gathered(three)

    @pl.when(inner)
    def _():
        gathered(three, range(4, 8))

    gate_up(three)
    ag_start(three)
    give(two, 0)
    give(two, 1)
    finish()
    down_other(three, 0)
    down_other(three, 1)
    down_own(three)
    give(three, 0)
    give(three, 1)
    down_other(z, 0)
    down_other(z, 1)
    down_own(z)
    combine_far(two * 2 + 0, first=True)
    combine_far(two * 2 + 1)
    combine_far(one * 2 + 0)
    combine_far(one * 2 + 1)
    give_own()
    combine(ep, res[z, pl.ds(pl.multiple_of(c * cap, cap), cap)])
    combine_far(other)
    combine_far(three * 2 + 0)
    combine_far(three * 2 + 1, last=True)

    for k in range(4):

        @pl.when((z + 1 < nz) & ((z == 0) | (k < 2)))
        def _():
            z_own(k, 1).wait_send()

        @pl.when((z > 0) & ((z + 1 == nz) | (k < 2)))
        def _():
            z_own(k, 0).wait_send()

    for k in range(4):
        w_copy(k).wait_send()

    own_copy(c).wait_send()

    @pl.when(ep + 1 < n_ep)
    def _():
        halo_copy().wait_send()

    for by in range(1, n_ep):
        ends_copy(by).wait_send()

    def drain(q, carry):
        for cc in range(2):
            ag_copy(q, cc).wait_send()
            rs_copy(q, cc).wait_send()

        @pl.when(q != z)
        def _():
            route_copy(q).wait_send()
            for kind in range(4, 6):
                x_copy(q, kind).wait_send()

        whole = inner & (q == block_at(2))

        @pl.when((q != z) & jnp.logical_not(whole))
        def _():
            for kind in range(4):
                x_copy(q, kind).wait_send()

        @pl.when(whole)
        def _():
            for kind in range(6, 8):
                x_copy(q, kind).wait_send()

        for k in range(2):

            @pl.when((q < z) & (z + 1 < nz))
            def _():
                z_copy(q, k, 1).wait_send()

            @pl.when((q > z) & (z > 0))
            def _():
                z_copy(q, k, 0).wait_send()

        for cc in range(2):

            @pl.when((q != z) | (c != cc))
            def _():
                ret_copy(q, cc).wait_send()

        return carry

    lax.fori_loop(0, nz, drain, 0)


def hand_kernel(a_in, b_in, a_out, b_out, sem):
    copies = [
        pltpu.make_async_copy(a_in, a_out, sem.at[0]),
        pltpu.make_async_copy(b_in, b_out, sem.at[1]),
    ]
    for copy in copies:
        copy.start()
    for copy in copies:
        copy.wait()


def hand_over(a, b):
    hbm = pl.BlockSpec(memory_space=pltpu.HBM)
    vmem = pl.BlockSpec(memory_space=pltpu.VMEM)
    return pl.pallas_call(
        hand_kernel,
        out_shape=tuple(jax.ShapeDtypeStruct(v.shape, v.dtype) for v in (a, b)),
        in_specs=[vmem, vmem],
        out_specs=(hbm, hbm),
        scratch_shapes=[pltpu.SemaphoreType.DMA((2,))],
        compiler_params=pltpu.CompilerParams(vmem_limit_bytes=4 << 20),
        name="hand",
    )(a, b)


def both_fused(
    mix_in,
    mix_gain,
    w_in_x,
    w_in_y,
    conv_taps,
    recur_gate_w,
    input_gate_w,
    decay_logit,
    decay_shift,
    moe_in,
    moe_gain,
    routes,
    route_weight,
    expert_gate,
    expert_up,
    expert_down,
):
    n_ep = lax.axis_size("ep")
    nz = n_ep // 2
    rows, features = moe_in.shape
    share = features // 4
    ff_dev, out_dev = expert_gate.shape[2], expert_down.shape[2]
    width = w_in_x.shape[1]
    cap = 2 * rows * routes.shape[1] // n_ep
    pair = 2 * cap
    vmem = pl.BlockSpec(memory_space=pltpu.VMEM)
    hbm = pl.BlockSpec(memory_space=pltpu.HBM)
    dma = pltpu.SemaphoreType.DMA
    flops = 2 * n_ep * cap * features * (2 * ff_dev + out_dev)
    results = pl.pallas_call(
        functools.partial(both_kernel, cap),
        out_shape=(pltpu.VMEM((rows, width), BF16), pltpu.VMEM((rows, out_dev), BF16)),
        in_specs=[hbm] * 6 + [vmem] * 3 + [hbm] + [vmem] * 3 + [hbm] * 3,
        out_specs=(vmem, vmem),
        scratch_shapes=[
            pltpu.VMEM((rows, features), BF16),
            pltpu.VMEM((nz, 4, rows, share), BF16),
            pltpu.VMEM((nz, pair, features), BF16),
            pltpu.VMEM((nz, 4, cap, share), BF16),
            pltpu.VMEM((cap, features), BF16),
            pltpu.VMEM((nz, pair, rows), BF16),
            pltpu.VMEM((nz, pair, 2 * ff_dev), BF16),
            pltpu.VMEM((nz, pair, out_dev), BF16),
            pltpu.VMEM((nz, pair, out_dev), BF16),
            pltpu.VMEM((nz, pair, out_dev), F32),
            pltpu.VMEM((nz, pair, out_dev), BF16),
            pltpu.VMEM((n_ep, cap, out_dev), BF16),
            pltpu.VMEM((nz, 2, rows), jnp.int32),
            pltpu.VMEM((n_ep, rows, cap), BF16),
            pltpu.VMEM((n_ep, rows, 128), F32),
            pltpu.VMEM((rows, out_dev), F32),
            pltpu.VMEM(expert_gate.shape[1:], BF16),
            pltpu.VMEM(expert_up.shape[1:], BF16),
            pltpu.VMEM((2, 2 * ff_dev, out_dev), BF16),
            dma((11,)),
            dma((2, nz)),
            dma((2, 4, nz)),
            dma((4, nz)),
            dma((2, 4)),
            dma((8, nz)),
            dma((8, nz)),
            dma((2, n_ep)),
            dma((2, n_ep)),
            dma((2, n_ep)),
            pltpu.VMEM(mix_in.shape, BF16),
            pltpu.VMEM(w_in_x.shape, BF16),
            pltpu.VMEM(w_in_y.shape, BF16),
            pltpu.VMEM(recur_gate_w.shape, BF16),
            pltpu.VMEM(input_gate_w.shape, BF16),
            pltpu.VMEM((rows, width), F32),
            pltpu.VMEM((16 + rows, width), BF16),
            pltpu.VMEM((rows, width), BF16),
            pltpu.VMEM((rows, width), F32),
            pltpu.VMEM((rows, width), F32),
            pltpu.VMEM((n_ep, 2, width), F32),
            dma((2,)),
            dma((2, n_ep)),
        ],
        compiler_params=pltpu.CompilerParams(
            collective_id=0, has_side_effects=True, vmem_limit_bytes=66000000
        ),
        cost_estimate=pl.CostEstimate(flops=flops, bytes_accessed=16 << 20, transcendentals=0),
        name="both",
    )(
        mix_in,
        w_in_x,
        w_in_y,
        recur_gate_w,
        input_gate_w,
        decay_shift,
        mix_gain[None, :],
        conv_taps,
        decay_logit[None, :],
        moe_in,
        moe_gain[None, :],
        routes.T,
        route_weight.T,
        expert_gate,
        expert_up,
        expert_down,
    )
    return hand_over(*results)


def from_behind(value, axis, by):
    count = lax.axis_size(axis)
    pairs = [(i, i + by) for i in range(count) if 0 <= i + by < count]
    return lax.ppermute(value, axis, pairs)


def entering(value, axis, combine, identity):
    count, index = (lax.axis_size(axis), lax.axis_index(axis))
    everything = jax.tree.map(lambda part: lax.all_gather(part, axis), value)
    start = jax.tree.map(
        lambda part, zero: jnp.broadcast_to(jnp.asarray(zero, part.dtype), part.shape),
        value,
        identity,
    )

    def hop(k, before):
        reached = k < index
        new = combine(before, jax.tree.map(lambda part: part[k], everything))
        return jax.tree.map(lambda a, b: jnp.where(reached, a, b), new, before)

    return lax.fori_loop(0, count, hop, start)


def norm_rows(rows, gain):
    widened = rows.astype(jnp.float32)
    scaled = widened * lax.rsqrt(jnp.mean(widened * widened, axis=-1, keepdims=True) + epsilon)
    return (scaled * gain[None, :]).astype(jnp.bfloat16)


def link(earlier, later):
    return (earlier[0] * later[0], later[0] * earlier[1] + later[1])


def fits_fused(moe_in, routes):
    n_ep = lax.axis_size("ep")
    gathered = n_ep * moe_in.size * moe_in.dtype.itemsize
    even = n_ep == 4 * routes.shape[1] == 2 * len(block_order)
    return lax.axis_size("tp") == 4 and even and gathered <= (16 << 20)


def moe_staged(moe_in, moe_gain, routes, route_weight, expert_gate, expert_up, expert_down):
    moe_rows = norm_rows(moe_in, moe_gain)
    token_count = moe_rows.shape[0]
    feature_count = moe_rows.shape[1]
    choose_count = routes.shape[1]
    expert_count = lax.axis_size("ep")
    capacity = 2 * token_count * choose_count // expert_count
    slot_total = expert_count * capacity
    expert_ids = routes.reshape(-1)
    onehot = (expert_ids[:, None] == jnp.arange(expert_count, dtype=jnp.int32)[None, :]).astype(
        jnp.int32
    )
    slot_rank = jnp.sum(jnp.cumsum(onehot, axis=0) * onehot, axis=1) - 1
    slot_index = expert_ids * capacity + slot_rank
    token_index = jnp.repeat(jnp.arange(token_count, dtype=jnp.int32), choose_count)
    slot_owner = jnp.full((slot_total,), token_count, jnp.int32).at[slot_index].set(token_index)
    padded_rows = jnp.concatenate([moe_rows, jnp.zeros((1, feature_count), jnp.bfloat16)], axis=0)
    outgoing = padded_rows[slot_owner].reshape(expert_count, capacity, feature_count)
    column_width = feature_count // lax.axis_size("tp")
    own_columns = lax.dynamic_slice_in_dim(
        outgoing, lax.axis_index("tp") * column_width, column_width, 2
    )
    incoming = lax.all_to_all(own_columns, "ep", split_axis=0, concat_axis=0, tiled=True)
    piece = lax.all_gather(incoming, "tp", axis=2, tiled=True)
    flat_rows = piece.reshape(slot_total, piece.shape[2])
    gate_rows = expert_gate[0]
    up_rows = expert_up[0]
    gate_proj = jnp.dot(flat_rows, gate_rows, preferred_element_type=jnp.float32)
    up_proj = jnp.dot(flat_rows, up_rows, preferred_element_type=jnp.float32)
    hidden = (jax.nn.silu(gate_proj) * up_proj).astype(jnp.bfloat16)
    down_rows = expert_down[0]
    columns = jnp.dot(
        lax.all_gather(hidden, "tp", axis=1, tiled=True),
        down_rows,
        preferred_element_type=jnp.float32,
    )
    results = columns.astype(jnp.bfloat16).reshape(expert_count, capacity, expert_down.shape[2])
    returned = lax.all_to_all(results, "ep", split_axis=0, concat_axis=0, tiled=True).reshape(
        slot_total, expert_down.shape[2]
    )
    picked = (
        returned[slot_index]
        .astype(jnp.float32)
        .reshape(token_count, choose_count, expert_down.shape[2])
    )
    route_share = route_weight / jnp.sum(route_weight, axis=1, keepdims=True)
    moe_out = jnp.sum(route_share[:, :, None] * picked, axis=1).astype(jnp.bfloat16)
    return moe_out


def staged(
    mix_in,
    mix_gain,
    w_in_x,
    w_in_y,
    conv_taps,
    recur_gate_w,
    input_gate_w,
    decay_logit,
    decay_shift,
    moe_in,
    moe_gain,
    routes,
    route_weight,
    expert_gate,
    expert_up,
    expert_down,
):
    row_count = mix_in.shape[0]
    width_dev = w_in_x.shape[1]
    heads_dev = recur_gate_w.shape[0]
    block_size = recur_gate_w.shape[1]
    tap_count = conv_taps.shape[0]
    mixer_rows = norm_rows(mix_in, mix_gain)
    x_branch = jnp.dot(mixer_rows, w_in_x, preferred_element_type=jnp.float32).astype(jnp.bfloat16)
    y_branch = jnp.dot(mixer_rows, w_in_y, preferred_element_type=jnp.float32).astype(jnp.bfloat16)
    previous = from_behind(x_branch[row_count - (tap_count - 1) :], "ep", 1)
    padded = jnp.concatenate([previous, x_branch], axis=0)
    conv_sum = jnp.zeros((row_count, width_dev), jnp.float32)
    for tap_index in range(tap_count):
        conv_sum = conv_sum + conv_taps[tap_index][None, :] * padded[
            tap_index : tap_index + row_count
        ].astype(jnp.float32)
    x_conv = conv_sum.astype(jnp.bfloat16)
    heads_in = x_conv.reshape(row_count, heads_dev, block_size)
    gate_a = jnp.einsum(
        "thi,hij->thj", heads_in, recur_gate_w, preferred_element_type=jnp.float32
    ).reshape(row_count, width_dev)
    gate_x = jnp.einsum(
        "thi,hij->thj", heads_in, input_gate_w, preferred_element_type=jnp.float32
    ).reshape(row_count, width_dev)
    log_decay = (
        -lru_scale * jax.nn.sigmoid(gate_a) * jax.nn.softplus(-decay_logit)[None, :] + decay_shift
    )
    lru_drive = (
        jnp.sqrt(-jnp.expm1(2.0 * log_decay)) * jax.nn.sigmoid(gate_x) * x_conv.astype(jnp.float32)
    )
    through, local_state = lax.associative_scan(link, (jnp.exp(log_decay), lru_drive), axis=0)
    identity = (jnp.ones((width_dev,), jnp.float32), jnp.zeros((width_dev,), jnp.float32))
    carried = entering((through[row_count - 1], local_state[row_count - 1]), "ep", link, identity)
    lru_state = local_state + through * carried[1][None, :]
    mixer_out = (lru_state * jax.nn.gelu(y_branch.astype(jnp.float32))).astype(jnp.bfloat16)
    moe_out = moe_staged(
        moe_in, moe_gain, routes, route_weight, expert_gate, expert_up, expert_down
    )
    return (mixer_out, moe_out)


def local(*args):
    return (both_fused if fits_fused(args[9], args[11]) else staged)(*args)


def solution(mesh):
    placed = (
        P("ep", None),
        P(),
        P(None, "tp"),
        P(None, "tp"),
        P(None, "tp"),
        P("tp", None, None),
        P("tp", None, None),
        P("tp"),
        P("ep", "tp"),
        P("ep", None),
        P(),
        P("ep", None),
        P("ep", None),
        P("ep", None, "tp"),
        P("ep", None, "tp"),
        P("ep", None, "tp"),
    )
    return jax.shard_map(
        local, mesh=mesh, in_specs=placed, out_specs=(P("ep", "tp"), P("ep", "tp")), check_vma=False
    )
```

```python
import functools

import jax
import jax.numpy as jnp
from jax import lax
from jax.experimental import pallas as pl
from jax.experimental.pallas import tpu as pltpu
from jax.sharding import PartitionSpec as P

epsilon = 1e-06
lru_scale = 8.0
MESH = pl.DeviceIdType.MESH
F32 = jnp.float32
BF16 = jnp.bfloat16


block_order = ((1, 2, 3), (2, 3, 0), (1, 0, 3), (2, 1, 0))


def one_minus_exp(value):
    series = jnp.full_like(value, 1.0 / 9.0)
    for k in range(8, 1, -1):
        series = (1.0 + value * series) * (1.0 / k)
    series = 1.0 + value * series
    return jnp.where(value > -0.5, -value * series, 1.0 - jnp.exp(value))


def soft_plus(value):
    small = jnp.exp(-jnp.abs(value))
    series = jnp.full_like(small, 1.0 / 7.0)
    for k in range(6, 0, -1):
        series = 1.0 / k - small * series
    wide = jnp.where(small < 0.05, small * series, jnp.log(1.0 + small))
    return jnp.maximum(value, 0.0) + wide


def both_kernel(
    cap,
    mix_hbm,
    wx_hbm,
    wy_hbm,
    ga_hbm,
    gx_hbm,
    shift_hbm,
    mix_gain_hbm,
    taps_hbm,
    logit_hbm,
    moe_hbm,
    gain_hbm,
    rt_hbm,
    rw_hbm,
    gate_hbm,
    up_hbm,
    down_hbm,
    mix_ref,
    out_ref,
    mix_gain_ref,
    taps_ref,
    logit_ref,
    gain_ref,
    rt_row,
    rw_row,
    small_sem,
    nrm,
    tok,
    xs,
    stage,
    own_stage,
    picks,
    hid,
    psend,
    precv,
    pown,
    res,
    ret,
    routes_all,
    comb,
    part,
    total,
    gw,
    uw,
    w2,
    load_sem,
    rt_sem,
    z_send,
    z_recv,
    w_sem,
    x_send,
    x_recv,
    push_sem,
    ag_sem,
    rs_sem,
    ret_sem,
    mixv,
    wx,
    wy,
    gaw,
    gxw,
    shiftv,
    xb,
    yb,
    av,
    bv,
    ends,
    halo_sem,
    ends_sem,
):
    n_ep = lax.axis_size("ep")
    nz = n_ep // 2
    ep = lax.axis_index("ep")
    t = lax.axis_index("tp")
    z, c = ep // 2, ep % 2
    y, x = t // 2, t % 2
    xp, yp, dg = y * 2 + (1 - x), (1 - y) * 2 + x, 3 - t
    pa, pb = jnp.where(c == 0, xp, yp), jnp.where(c == 0, yp, xp)
    other = z * 2 + (1 - c)
    rows, share = tok.shape[2], tok.shape[3]
    inner = (z > 0) & (z + 1 < nz)
    outer = jnp.logical_not(inner)
    shares = (t, dg, xp, yp)

    def block_at(s):
        q = jnp.int32(0)
        for zz in range(nz):
            q = jnp.where(z == zz, block_order[zz][s], q)
        return q

    def remote(src, dst, send, recv, where):
        return pltpu.make_async_remote_copy(
            src_ref=src,
            dst_ref=dst,
            send_sem=send,
            recv_sem=recv,
            device_id=where,
            device_id_type=MESH,
        )

    span = w2.shape[2]
    half = w2.shape[1] // 2

    def down_rows(k):
        return down_hbm.at[0, pl.ds(pl.multiple_of(k * half, half), half)]

    loads = [
        pltpu.make_async_copy(moe_hbm, nrm, load_sem.at[0]),
        pltpu.make_async_copy(gate_hbm.at[0], gw, load_sem.at[1]),
        pltpu.make_async_copy(up_hbm.at[0], uw, load_sem.at[2]),
        pltpu.make_async_copy(mix_hbm, mixv, load_sem.at[3]),
        pltpu.make_async_copy(wx_hbm, wx, load_sem.at[4]),
        pltpu.make_async_copy(wy_hbm, wy, load_sem.at[5]),
        pltpu.make_async_copy(ga_hbm, gaw, load_sem.at[6]),
        pltpu.make_async_copy(gx_hbm, gxw, load_sem.at[7]),
        pltpu.make_async_copy(shift_hbm, shiftv, load_sem.at[8]),
        pltpu.make_async_copy(down_rows(t), w2.at[0, pl.ds(0, half)], load_sem.at[9]),
        pltpu.make_async_copy(down_rows(pa), w2.at[0, pl.ds(half, half)], load_sem.at[10]),
    ]
    small = [
        pltpu.make_async_copy(gain_hbm, gain_ref, small_sem.at[0]),
        pltpu.make_async_copy(rt_hbm, rt_row, small_sem.at[1]),
        pltpu.make_async_copy(rw_hbm, rw_row, small_sem.at[2]),
        pltpu.make_async_copy(mix_gain_hbm, mix_gain_ref, small_sem.at[3]),
        pltpu.make_async_copy(taps_hbm, taps_ref, small_sem.at[4]),
        pltpu.make_async_copy(logit_hbm, logit_ref, small_sem.at[5]),
    ]
    loads[0].start()
    for copy in small[:2]:
        copy.start()
    barrier = pltpu.get_barrier_semaphore()
    for by in range(1, n_ep):
        pl.semaphore_signal(
            barrier, inc=1, device_id={"ep": (ep + by) % n_ep}, device_id_type=MESH
        )
    for peer in (xp, yp):
        for near in (ep, other):
            pl.semaphore_signal(
                barrier, inc=1, device_id={"ep": near, "tp": peer}, device_id_type=MESH
            )
    for copy in small[2:] + loads[3:6] + loads[1:3] + loads[6:]:
        copy.start()

    def columns(k):
        return pl.ds(pl.multiple_of(k * share, share), share)

    def z_slot(q, k):
        return q * 2 + k if k < 2 else nz * 2 + k - 2

    def z_own(k, up):
        return remote(
            nrm.at[:, columns(shares[k])],
            tok.at[z, k],
            z_send.at[z],
            z_recv.at[z_slot(z, k)],
            {"ep": ep + (2 if up else -2)},
        )

    def z_copy(q, k, up):
        return remote(
            tok.at[q, k],
            tok.at[q, k],
            z_send.at[q],
            z_recv.at[z_slot(q, k)],
            {"ep": ep + (2 if up else -2)},
        )

    def route_copy(q):
        return remote(rt_row, routes_all.at[z], rt_sem.at[nz], rt_sem.at[z], {"ep": q * 2 + c})

    def w_copy(k):
        piece = half // 2
        first = (pb, dg)[k // 2] * half + k % 2 * piece
        return remote(
            down_hbm.at[0, pl.ds(pl.multiple_of(first, piece), piece)],
            w2.at[1, pl.ds(k * piece, piece)],
            w_sem.at[0],
            w_sem.at[1],
            {"tp": pb},
        )

    def xs_part(q, block, k):
        return xs.at[q, pl.ds(pl.multiple_of(block * cap, cap), cap), columns(k)]

    def x_copy(q, kind):
        to = (xp, yp, xp, yp, t, t, t, t)[kind]
        near = ep if kind < 2 else other
        src = xs_part(q, c, t) if kind < 2 else stage.at[q, max(kind - 4, 0)]
        return remote(
            src,
            xs_part(q, c, shares[max(kind - 4, 0)]),
            x_send.at[q],
            x_recv.at[q],
            {"ep": near, "tp": to},
        )

    def x_all(q, count):
        part = xs.at[q, pl.ds(0, count * cap // 4)]
        return remote(part, part, x_send.at[q], x_recv.at[q], {"ep": other})

    def own_copy(block):
        return remote(
            own_stage,
            xs.at[z, pl.ds(pl.multiple_of(block * cap, cap), cap)],
            x_send.at[z],
            x_recv.at[z],
            {"ep": other},
        )

    def ag_copy(q, cc):
        at, sem = pl.ds(cc * cap, cap), q * 2 + cc
        return remote(
            hid.at[q, at, pl.ds(0, half)],
            hid.at[q, at, pl.ds(half, half)],
            push_sem.at[0],
            ag_sem.at[sem],
            {"tp": pa},
        )

    def rs_copy(q, cc):
        at, sem = pl.ds(cc * cap, cap), q * 2 + cc
        return remote(
            psend.at[q, at], precv.at[q, at], push_sem.at[0], rs_sem.at[sem], {"tp": pb}
        )

    def ret_copy(q, cc):
        return remote(
            res.at[q, pl.ds(cc * cap, cap)],
            ret.at[ep],
            push_sem.at[1],
            ret_sem.at[ep],
            {"ep": q * 2 + cc},
        )

    def arrive(q, k):
        z_copy(q, k, 1).wait_recv()
        if k < 2:

            @pl.when((q < z) & (z + 1 < nz))
            def _():
                z_copy(q, k, 1).start()

            @pl.when((q > z) & (z > 0))
            def _():
                z_copy(q, k, 0).start()

    def make_picks(q, named):
        lane = lax.broadcasted_iota(jnp.int32, (8, rows), 0)
        which = z * 2 + jnp.where(lane == 0, c, 1 - c)
        mask = jnp.where((named[0:1] == which) | (named[1:2] == which), 1.0, 0.0)
        before = jnp.where(
            lax.broadcasted_iota(jnp.int32, (rows, rows), 0)
            < lax.broadcasted_iota(jnp.int32, (rows, rows), 1),
            1.0,
            0.0,
        ).astype(BF16)
        rank = jnp.dot(mask.astype(BF16), before, preferred_element_type=F32)
        key = jnp.where(mask > 0.5, rank, -1.0)
        seat = lax.broadcasted_iota(jnp.int32, (cap, rows), 0).astype(F32)
        for k in range(2):
            picks[q, k * cap : (k + 1) * cap] = jnp.where(
                seat == key[k : k + 1], 1.0, 0.0
            ).astype(BF16)

    def pick_own():
        for k in range(4):
            at = pl.ds(k * share, share)
            got = jnp.dot(picks[z], nrm[:, at], preferred_element_type=F32).astype(BF16)
            xs[z, pl.ds(pl.multiple_of(c * cap, cap), cap), at] = got[:cap]
            own_stage[:, at] = got[cap:]
        own_copy(c).start()

    def pick(q, k, whole=False):
        got = jnp.dot(picks[q], tok[q, k], preferred_element_type=F32).astype(BF16)
        xs[q, pl.ds(pl.multiple_of(c * cap, cap), cap), columns(shares[k])] = got[:cap]
        stage[q, k] = got[cap:]
        for kind in range(5) if k == 0 and not whole else (4 + k,):
            x_copy(q, kind).start()

    def gate_up(q):
        tile = 256

        @pl.loop(0, gw.shape[1] // tile)
        def _(j):
            cols = pl.ds(pl.multiple_of(j * tile, tile), tile)
            g = jnp.dot(xs[q], gw[:, cols], preferred_element_type=F32)
            u = jnp.dot(xs[q], uw[:, cols], preferred_element_type=F32)
            hid[q, :, cols] = (jax.nn.silu(g) * u).astype(BF16)

    def gathered(q, count=6):
        x_all(q, count).wait_recv()

    def ag_start(q):
        for cc in range(2):
            ag_copy(q, cc).start()

    def down_other(q, cc):
        tile = 256
        at = pl.ds(cc * cap, cap)
        ag_copy(q, cc).wait_recv()

        @pl.loop(0, span // tile)
        def _(j):
            cols = pl.ds(pl.multiple_of(j * tile, tile), tile)
            psend[q, at, cols] = jnp.dot(
                hid[q, at], w2[1, :, cols], preferred_element_type=F32
            ).astype(BF16)

        rs_copy(q, cc).start()

    def down_own(q):
        tile = 256

        @pl.loop(0, span // tile)
        def _(j):
            cols = pl.ds(pl.multiple_of(j * tile, tile), tile)
            pown[q, :, cols] = jnp.dot(hid[q], w2[0, :, cols], preferred_element_type=F32)

    def give(q, cc):
        at = pl.ds(cc * cap, cap)
        rs_copy(q, cc).wait_recv()
        res[q, at] = (pown[q, at] + precv[q, at].astype(F32)).astype(BF16)
        ret_copy(q, cc).start()

    def give_own():
        for cc in range(2):
            at = pl.ds(cc * cap, cap)
            rs_copy(z, cc).wait_recv()
            res[z, at] = (pown[z, at] + precv[z, at].astype(F32)).astype(BF16)

            @pl.when(c != cc)
            def _():
                ret_copy(z, cc).start()

    pad = xb.shape[0] - rows

    def halo_copy():
        return remote(
            xb.at[pl.ds(rows, pad)],
            xb.at[pl.ds(0, pad)],
            halo_sem.at[0],
            halo_sem.at[1],
            {"ep": ep + 1},
        )

    def ends_copy(by):
        return remote(
            ends.at[ep],
            ends.at[ep],
            ends_sem.at[0],
            ends_sem.at[1],
            {"ep": (ep + by) % n_ep},
        )

    def ends_all():
        part = ends.at[pl.ds(0, n_ep - 1)]
        return remote(part, part, ends_sem.at[0], ends_sem.at[1], {"ep": other})

    def norm(buffer, gain):
        strip = 64

        @pl.loop(0, rows // strip)
        def _(i):
            at = pl.ds(pl.multiple_of(i * strip, strip), strip)
            wide = buffer[at, :].astype(F32)
            scale = lax.rsqrt(jnp.mean(wide * wide, axis=-1, keepdims=True) + epsilon)
            buffer[at, :] = (wide * scale * gain[...]).astype(BF16)

    def project():
        for k in range(3, 6):
            loads[k].wait()
        norm(mixv, mix_gain_ref)
        tile = 256

        @pl.loop(0, wx.shape[1] // tile)
        def _(j):
            cols = pl.ds(pl.multiple_of(j * tile, tile), tile)
            xb[pl.ds(pad, rows), cols] = jnp.dot(
                mixv[...], wx[:, cols], preferred_element_type=F32
            ).astype(BF16)
            yb[:, cols] = jnp.dot(mixv[...], wy[:, cols], preferred_element_type=F32).astype(BF16)

        @pl.when(ep + 1 < n_ep)
        def _():
            halo_copy().start()

        @pl.when(ep == 0)
        def _():
            xb[pl.ds(0, pad), :] = jnp.zeros((pad, xb.shape[1]), BF16)

    def drives_ready():
        for k in range(6, 9):
            loads[k].wait()

        @pl.when(ep > 0)
        def _():
            halo_copy().wait_recv()

    def drives(heads):
        taps = taps_ref.shape[0]
        size = gaw.shape[1]
        for h in heads:
            cols = pl.ds(h * size, size)
            wide = xb[:, cols].astype(F32)
            conv = jnp.zeros((rows, size), F32)
            for k in range(taps):
                first_row = pad - (taps - 1) + k
                conv = conv + taps_ref[k : k + 1, cols] * wide[first_row : first_row + rows]
            x_conv = conv.astype(BF16)
            gate_a = jnp.dot(x_conv, gaw[h], preferred_element_type=F32)
            gate_x = jnp.dot(x_conv, gxw[h], preferred_element_type=F32)
            log_decay = (
                -lru_scale * jax.nn.sigmoid(gate_a) * soft_plus(-logit_ref[:, cols])
                + shiftv[:, cols]
            )
            av[:, cols] = jnp.exp(log_decay)
            bv[:, cols] = (
                jnp.sqrt(one_minus_exp(2.0 * log_decay))
                * jax.nn.sigmoid(gate_x)
                * x_conv.astype(F32)
            )

    def recur():
        width = av.shape[1]
        row = lax.broadcasted_iota(jnp.int32, (8, width), 0)

        def group(i, carry):
            at = pl.ds(pl.multiple_of(i * 8, 8), 8)
            a, b = av[at, :], bv[at, :]
            for by in (1, 2, 4):
                a_past, b_past = pltpu.roll(a, by, 0), pltpu.roll(b, by, 0)
                b = jnp.where(row >= by, a * b_past + b, b)
                a = jnp.where(row >= by, a * a_past, a)
            b = a * carry[1] + b
            a = a * carry[0]
            av[at, :] = a
            bv[at, :] = b
            return (a[7:8], b[7:8])

        through, state = lax.fori_loop(
            0, rows // 8, group, (jnp.ones((1, width), F32), jnp.zeros((1, width), F32))
        )
        ends[ep, 0:1] = through
        ends[ep, 1:2] = state
        for by in range(1, n_ep):
            ends_copy(by).start()

    def finish():
        carried = jnp.zeros((1, av.shape[1]), F32)
        ends_all().wait_recv()
        for k in range(n_ep):
            entered = ends[k, 0:1] * carried + ends[k, 1:2]
            carried = jnp.where(k < ep, entered, carried)
        strip = 32

        @pl.loop(0, rows // strip)
        def _(i):
            at = pl.ds(pl.multiple_of(i * strip, strip), strip)
            state = bv[at, :] + av[at, :] * carried
            mix_ref[at, :] = (state * jax.nn.gelu(yb[at, :].astype(F32))).astype(BF16)

    def drain_early():
        part = xs.at[0]
        remote(part, part, z_send.at[z], z_recv.at[0], {"ep": other}).wait_send()
        remote(part, part, w_sem.at[0], w_sem.at[1], {"ep": other}).wait_send()
        own_copy(c).wait_send()
        ends_all().wait_send()
        part = routes_all.at[pl.ds(0, nz - 1)]
        remote(part, part, rt_sem.at[nz], rt_sem.at[0], {"ep": other}).wait_send()

        @pl.when(ep + 1 < n_ep)
        def _():
            halo_copy().wait_send()

        def drain_one(q, carry):
            whole = inner & (q == block_at(2))

            @pl.when((q != z) & jnp.logical_not(whole))
            def _():
                x_all(q, 6).wait_send()

            @pl.when(whole)
            def _():
                x_all(q, 4).wait_send()

            @pl.when((q != z) & inner)
            def _():
                part = tok.at[q, pl.ds(0, 2)]
                remote(part, part, z_send.at[q], z_recv.at[0], {"ep": other}).wait_send()

            return carry

        lax.fori_loop(0, nz, drain_one, 0)

    def make_combine():
        weights = rw_row[...]
        sides = jnp.concatenate(
            [
                rt_row[...].astype(F32),
                weights / (weights[0:1] + weights[1:2]),
                jnp.zeros((124, rows), F32),
            ],
            axis=0,
        ).T
        one, two = sides[:, 0:1].astype(jnp.int32), sides[:, 1:2].astype(jnp.int32)
        lane = lax.broadcasted_iota(jnp.int32, (rows, 128), 1)
        mask = jnp.where((one == lane) | (two == lane), 1.0, 0.0)
        before = jnp.where(
            lax.broadcasted_iota(jnp.int32, (rows, rows), 1)
            < lax.broadcasted_iota(jnp.int32, (rows, rows), 0),
            1.0,
            0.0,
        ).astype(BF16)
        rank = jnp.dot(before, mask.astype(BF16), preferred_element_type=F32)
        key = jnp.where(mask > 0.5, rank, -1.0)
        part_one, part_two = sides[:, 2:3], sides[:, 3:4]
        seat = lax.broadcasted_iota(jnp.int32, (rows, cap), 1).astype(F32)
        for e in range(n_ep):
            comb[e] = jnp.where(seat == key[:, e : e + 1], 1.0, 0.0).astype(BF16)
            part[e] = jnp.broadcast_to(
                jnp.where(one == e, part_one, 0.0) + jnp.where(two == e, part_two, 0.0),
                (rows, 128),
            )

    def combine(e, rows_in, first=False, last=False):
        got = jnp.dot(comb[e], rows_in, preferred_element_type=F32)
        for j in range(got.shape[1] // 128):
            at = pl.ds(j * 128, 128)
            term = part[e] * got[:, j * 128 : (j + 1) * 128]
            if not first:
                term = total[:, at] + term
            if last:
                out_ref[:, at] = term.astype(BF16)
            else:
                total[:, at] = term

    def ret_wait(e):
        remote(
            res.at[0, pl.ds(0, cap)], ret.at[e], push_sem.at[1], ret_sem.at[e], {"ep": other}
        ).wait_recv()

    def combine_far(e, first=False, last=False):
        ret_wait(e)
        combine(e, ret[e], first, last)

    loads[0].wait()
    for copy in small[:2]:
        copy.wait()
    norm(nrm, gain_ref)
    pl.semaphore_wait(barrier, n_ep + 3)
    for q in range(nz):

        @pl.when(q != z)
        def _():
            route_copy(q).start()

    for k in range(4):

        @pl.when((z + 1 < nz) & ((z == 0) | (k < 2)))
        def _():
            z_own(k, 1).start()

        @pl.when((z > 0) & ((z + 1 == nz) | (k < 2)))
        def _():
            z_own(k, 0).start()

    for k in range(3):
        w_copy(k).start()
    make_picks(z, rt_row[...])
    pick_own()
    for copy in small[2:]:
        copy.wait()
    one, two, three = block_at(0), block_at(1), block_at(2)
    for q in (one, two, three):
        remote(
            rt_row, routes_all.at[q], rt_sem.at[nz], rt_sem.at[q], {"ep": q * 2 + c}
        ).wait_recv()
        make_picks(q, routes_all[q])
    project()
    own_copy(1 - c).wait_recv()
    for k in range(1, 3):
        loads[k].wait()
    gate_up(z)
    arrive(one, 0)
    pick(one, 0)
    w_copy(3).start()

    @pl.when(inner)
    def _():
        arrive(three, 0)

    make_combine()
    arrive(one, 1)
    pick(one, 1)

    @pl.when(inner)
    def _():
        arrive(three, 1)

    gathered(one)
    gate_up(one)
    ag_start(one)
    arrive(two, 0)
    pick(two, 0)
    for k in range(9, 11):
        loads[k].wait()
    remote(w2.at[1], w2.at[1], w_sem.at[0], w_sem.at[1], {"tp": pb}).wait_recv()
    down_other(one, 0)
    down_other(one, 1)
    down_own(one)
    arrive(two, 1)
    pick(two, 1)
    gathered(two)
    gate_up(two)
    ag_start(two)
    drives_ready()
    drives(range(0, 4))
    give(one, 0)
    give(one, 1)
    recur()

    @pl.when(outer)
    def _():
        arrive(three, 0)
        pick(three, 0)

    @pl.when(inner)
    def _():
        pick(three, 0, True)

    down_other(two, 0)
    ag_start(z)
    down_other(two, 1)
    down_own(two)

    @pl.when(outer)
    def _():
        arrive(three, 1)
        pick(three, 1)

    @pl.when(inner)
    def _():
        pick(three, 1)
        for k in range(2, 4):
            arrive(three, k)
            pick(three, k)


    @pl.when(outer)
    def _():
        gathered(three)

    @pl.when(inner)
    def _():
        gathered(three, 4)

    gate_up(three)
    ag_start(three)
    give(two, 0)
    give(two, 1)
    finish()
    down_other(three, 0)
    down_other(three, 1)
    down_own(three)
    give(three, 0)
    give(three, 1)
    down_other(z, 0)
    down_other(z, 1)
    down_own(z)
    combine_far(two * 2 + 0, first=True)
    combine_far(two * 2 + 1)
    combine_far(one * 2 + 0)
    combine_far(one * 2 + 1)
    give_own()
    combine(ep, res[z, pl.ds(pl.multiple_of(c * cap, cap), cap)])
    drain_early()
    combine_far(other)
    combine_far(three * 2 + 0)
    combine_far(three * 2 + 1, last=True)

    part = xs.at[pl.ds(0, 2)]
    remote(part, part, push_sem.at[0], ag_sem.at[0], {"ep": other}).wait_send()
    part = xs.at[0, pl.ds(0, (n_ep - 1) * cap // 4)]
    remote(part, part, push_sem.at[1], ag_sem.at[0], {"ep": other}).wait_send()


def hand_kernel(a_in, b_in, a_out, b_out, sem):
    copies = [
        pltpu.make_async_copy(a_in, a_out, sem.at[0]),
        pltpu.make_async_copy(b_in, b_out, sem.at[1]),
    ]
    for copy in copies:
        copy.start()
    for copy in copies:
        copy.wait()


def hand_over(a, b):
    hbm = pl.BlockSpec(memory_space=pltpu.HBM)
    vmem = pl.BlockSpec(memory_space=pltpu.VMEM)
    return pl.pallas_call(
        hand_kernel,
        out_shape=tuple(jax.ShapeDtypeStruct(v.shape, v.dtype) for v in (a, b)),
        in_specs=[vmem, vmem],
        out_specs=(hbm, hbm),
        scratch_shapes=[pltpu.SemaphoreType.DMA((2,))],
        compiler_params=pltpu.CompilerParams(vmem_limit_bytes=4 << 20),
        name="hand",
    )(a, b)


def both_fused(
    mix_in,
    mix_gain,
    w_in_x,
    w_in_y,
    conv_taps,
    recur_gate_w,
    input_gate_w,
    decay_logit,
    decay_shift,
    moe_in,
    moe_gain,
    routes,
    route_weight,
    expert_gate,
    expert_up,
    expert_down,
):
    n_ep = lax.axis_size("ep")
    nz = n_ep // 2
    rows, features = moe_in.shape
    share = features // 4
    ff_dev, out_dev = expert_gate.shape[2], expert_down.shape[2]
    width = w_in_x.shape[1]
    cap = 2 * rows * routes.shape[1] // n_ep
    pair = 2 * cap
    vmem = pl.BlockSpec(memory_space=pltpu.VMEM)
    hbm = pl.BlockSpec(memory_space=pltpu.HBM)
    dma = pltpu.SemaphoreType.DMA
    flops = 2 * n_ep * cap * features * (2 * ff_dev + out_dev)
    results = pl.pallas_call(
        functools.partial(both_kernel, cap),
        out_shape=(pltpu.VMEM((rows, width), BF16), pltpu.VMEM((rows, out_dev), BF16)),
        in_specs=[hbm] * 16,
        out_specs=(vmem, vmem),
        scratch_shapes=[
            pltpu.VMEM((1, features), F32),
            pltpu.VMEM(conv_taps.shape, F32),
            pltpu.VMEM((1, width), F32),
            pltpu.VMEM((1, features), F32),
            pltpu.VMEM(routes.shape[::-1], jnp.int32),
            pltpu.VMEM(routes.shape[::-1], F32),
            dma((6,)),
            pltpu.VMEM((rows, features), BF16),
            pltpu.VMEM((nz, 4, rows, share), BF16),
            pltpu.VMEM((nz, pair, features), BF16),
            pltpu.VMEM((nz, 4, cap, share), BF16),
            pltpu.VMEM((cap, features), BF16),
            pltpu.VMEM((nz, pair, rows), BF16),
            pltpu.VMEM((nz, pair, 2 * ff_dev), BF16),
            pltpu.VMEM((nz, pair, out_dev), BF16),
            pltpu.VMEM((nz, pair, out_dev), BF16),
            pltpu.VMEM((nz, pair, out_dev), F32),
            pltpu.VMEM((nz, pair, out_dev), BF16),
            pltpu.VMEM((n_ep, cap, out_dev), BF16),
            pltpu.VMEM((nz, 2, rows), jnp.int32),
            pltpu.VMEM((n_ep, rows, cap), BF16),
            pltpu.VMEM((n_ep, rows, 128), F32),
            pltpu.VMEM((rows, out_dev), F32),
            pltpu.VMEM(expert_gate.shape[1:], BF16),
            pltpu.VMEM(expert_up.shape[1:], BF16),
            pltpu.VMEM((2, 2 * ff_dev, out_dev), BF16),
            dma((11,)),
            dma((nz + 1,)),
            dma((nz,)),
            dma((2 * nz + 2,)),
            dma((2,)),
            dma((nz,)),
            dma((nz,)),
            dma((2,)),
            dma((n_ep,)),
            dma((n_ep,)),
            dma((n_ep,)),
            pltpu.VMEM(mix_in.shape, BF16),
            pltpu.VMEM(w_in_x.shape, BF16),
            pltpu.VMEM(w_in_y.shape, BF16),
            pltpu.VMEM(recur_gate_w.shape, BF16),
            pltpu.VMEM(input_gate_w.shape, BF16),
            pltpu.VMEM((rows, width), F32),
            pltpu.VMEM((16 + rows, width), BF16),
            pltpu.VMEM((rows, width), BF16),
            pltpu.VMEM((rows, width), F32),
            pltpu.VMEM((rows, width), F32),
            pltpu.VMEM((n_ep, 2, width), F32),
            dma((2,)),
            dma((2,)),
        ],
        compiler_params=pltpu.CompilerParams(
            collective_id=0, has_side_effects=True, vmem_limit_bytes=66000000
        ),
        cost_estimate=pl.CostEstimate(flops=flops, bytes_accessed=16 << 20, transcendentals=0),
        name="both",
    )(
        mix_in,
        w_in_x,
        w_in_y,
        recur_gate_w,
        input_gate_w,
        decay_shift,
        mix_gain[None, :],
        conv_taps,
        decay_logit[None, :],
        moe_in,
        moe_gain[None, :],
        routes.T,
        route_weight.T,
        expert_gate,
        expert_up,
        expert_down,
    )
    return hand_over(*results)


def from_behind(value, axis, by):
    count = lax.axis_size(axis)
    pairs = [(i, i + by) for i in range(count) if 0 <= i + by < count]
    return lax.ppermute(value, axis, pairs)


def entering(value, axis, combine, identity):
    count, index = (lax.axis_size(axis), lax.axis_index(axis))
    everything = jax.tree.map(lambda part: lax.all_gather(part, axis), value)
    start = jax.tree.map(
        lambda part, zero: jnp.broadcast_to(jnp.asarray(zero, part.dtype), part.shape),
        value,
        identity,
    )

    def hop(k, before):
        reached = k < index
        new = combine(before, jax.tree.map(lambda part: part[k], everything))
        return jax.tree.map(lambda a, b: jnp.where(reached, a, b), new, before)

    return lax.fori_loop(0, count, hop, start)


def norm_rows(rows, gain):
    widened = rows.astype(jnp.float32)
    scaled = widened * lax.rsqrt(jnp.mean(widened * widened, axis=-1, keepdims=True) + epsilon)
    return (scaled * gain[None, :]).astype(jnp.bfloat16)


def link(earlier, later):
    return (earlier[0] * later[0], later[0] * earlier[1] + later[1])


def fits_fused(moe_in, routes):
    n_ep = lax.axis_size("ep")
    gathered = n_ep * moe_in.size * moe_in.dtype.itemsize
    even = n_ep == 4 * routes.shape[1] == 2 * len(block_order)
    return lax.axis_size("tp") == 4 and even and gathered <= (16 << 20)


def moe_staged(moe_in, moe_gain, routes, route_weight, expert_gate, expert_up, expert_down):
    moe_rows = norm_rows(moe_in, moe_gain)
    token_count = moe_rows.shape[0]
    feature_count = moe_rows.shape[1]
    choose_count = routes.shape[1]
    expert_count = lax.axis_size("ep")
    capacity = 2 * token_count * choose_count // expert_count
    slot_total = expert_count * capacity
    expert_ids = routes.reshape(-1)
    onehot = (expert_ids[:, None] == jnp.arange(expert_count, dtype=jnp.int32)[None, :]).astype(
        jnp.int32
    )
    slot_rank = jnp.sum(jnp.cumsum(onehot, axis=0) * onehot, axis=1) - 1
    slot_index = expert_ids * capacity + slot_rank
    token_index = jnp.repeat(jnp.arange(token_count, dtype=jnp.int32), choose_count)
    slot_owner = jnp.full((slot_total,), token_count, jnp.int32).at[slot_index].set(token_index)
    padded_rows = jnp.concatenate([moe_rows, jnp.zeros((1, feature_count), jnp.bfloat16)], axis=0)
    outgoing = padded_rows[slot_owner].reshape(expert_count, capacity, feature_count)
    column_width = feature_count // lax.axis_size("tp")
    own_columns = lax.dynamic_slice_in_dim(
        outgoing, lax.axis_index("tp") * column_width, column_width, 2
    )
    incoming = lax.all_to_all(own_columns, "ep", split_axis=0, concat_axis=0, tiled=True)
    piece = lax.all_gather(incoming, "tp", axis=2, tiled=True)
    flat_rows = piece.reshape(slot_total, piece.shape[2])
    gate_rows = expert_gate[0]
    up_rows = expert_up[0]
    gate_proj = jnp.dot(flat_rows, gate_rows, preferred_element_type=jnp.float32)
    up_proj = jnp.dot(flat_rows, up_rows, preferred_element_type=jnp.float32)
    hidden = (jax.nn.silu(gate_proj) * up_proj).astype(jnp.bfloat16)
    down_rows = expert_down[0]
    columns = jnp.dot(
        lax.all_gather(hidden, "tp", axis=1, tiled=True),
        down_rows,
        preferred_element_type=jnp.float32,
    )
    results = columns.astype(jnp.bfloat16).reshape(expert_count, capacity, expert_down.shape[2])
    returned = lax.all_to_all(results, "ep", split_axis=0, concat_axis=0, tiled=True).reshape(
        slot_total, expert_down.shape[2]
    )
    picked = (
        returned[slot_index]
        .astype(jnp.float32)
        .reshape(token_count, choose_count, expert_down.shape[2])
    )
    route_share = route_weight / jnp.sum(route_weight, axis=1, keepdims=True)
    moe_out = jnp.sum(route_share[:, :, None] * picked, axis=1).astype(jnp.bfloat16)
    return moe_out


def staged(
    mix_in,
    mix_gain,
    w_in_x,
    w_in_y,
    conv_taps,
    recur_gate_w,
    input_gate_w,
    decay_logit,
    decay_shift,
    moe_in,
    moe_gain,
    routes,
    route_weight,
    expert_gate,
    expert_up,
    expert_down,
):
    row_count = mix_in.shape[0]
    width_dev = w_in_x.shape[1]
    heads_dev = recur_gate_w.shape[0]
    block_size = recur_gate_w.shape[1]
    tap_count = conv_taps.shape[0]
    mixer_rows = norm_rows(mix_in, mix_gain)
    x_branch = jnp.dot(mixer_rows, w_in_x, preferred_element_type=jnp.float32).astype(jnp.bfloat16)
    y_branch = jnp.dot(mixer_rows, w_in_y, preferred_element_type=jnp.float32).astype(jnp.bfloat16)
    previous = from_behind(x_branch[row_count - (tap_count - 1) :], "ep", 1)
    padded = jnp.concatenate([previous, x_branch], axis=0)
    conv_sum = jnp.zeros((row_count, width_dev), jnp.float32)
    for tap_index in range(tap_count):
        conv_sum = conv_sum + conv_taps[tap_index][None, :] * padded[
            tap_index : tap_index + row_count
        ].astype(jnp.float32)
    x_conv = conv_sum.astype(jnp.bfloat16)
    heads_in = x_conv.reshape(row_count, heads_dev, block_size)
    gate_a = jnp.einsum(
        "thi,hij->thj", heads_in, recur_gate_w, preferred_element_type=jnp.float32
    ).reshape(row_count, width_dev)
    gate_x = jnp.einsum(
        "thi,hij->thj", heads_in, input_gate_w, preferred_element_type=jnp.float32
    ).reshape(row_count, width_dev)
    log_decay = (
        -lru_scale * jax.nn.sigmoid(gate_a) * jax.nn.softplus(-decay_logit)[None, :] + decay_shift
    )
    lru_drive = (
        jnp.sqrt(-jnp.expm1(2.0 * log_decay)) * jax.nn.sigmoid(gate_x) * x_conv.astype(jnp.float32)
    )
    through, local_state = lax.associative_scan(link, (jnp.exp(log_decay), lru_drive), axis=0)
    identity = (jnp.ones((width_dev,), jnp.float32), jnp.zeros((width_dev,), jnp.float32))
    carried = entering((through[row_count - 1], local_state[row_count - 1]), "ep", link, identity)
    lru_state = local_state + through * carried[1][None, :]
    mixer_out = (lru_state * jax.nn.gelu(y_branch.astype(jnp.float32))).astype(jnp.bfloat16)
    moe_out = moe_staged(
        moe_in, moe_gain, routes, route_weight, expert_gate, expert_up, expert_down
    )
    return (mixer_out, moe_out)


def local(*args):
    return (both_fused if fits_fused(args[9], args[11]) else staged)(*args)


def solution(mesh):
    placed = (
        P("ep", None),
        P(),
        P(None, "tp"),
        P(None, "tp"),
        P(None, "tp"),
        P("tp", None, None),
        P("tp", None, None),
        P("tp"),
        P("ep", "tp"),
        P("ep", None),
        P(),
        P("ep", None),
        P("ep", None),
        P("ep", None, "tp"),
        P("ep", None, "tp"),
        P("ep", None, "tp"),
    )
    return jax.shard_map(
        local, mesh=mesh, in_specs=placed, out_specs=(P("ep", "tp"), P("ep", "tp")), check_vma=False
    )
```

```python
import functools

import jax
import jax.numpy as jnp
from jax import lax
from jax.experimental import pallas as pl
from jax.experimental.pallas import tpu as pltpu
from jax.sharding import PartitionSpec as P

epsilon = 1e-06
lru_scale = 8.0
MESH = pl.DeviceIdType.MESH
F32 = jnp.float32
BF16 = jnp.bfloat16


block_order = ((1, 2, 3), (2, 3, 0), (1, 0, 3), (2, 1, 0))


def one_minus_exp(value):
    series = jnp.full_like(value, 1.0 / 9.0)
    for k in range(8, 1, -1):
        series = (1.0 + value * series) * (1.0 / k)
    series = 1.0 + value * series
    return jnp.where(value > -0.5, -value * series, 1.0 - jnp.exp(value))


def soft_plus(value):
    small = jnp.exp(-jnp.abs(value))
    series = jnp.full_like(small, 1.0 / 7.0)
    for k in range(6, 0, -1):
        series = 1.0 / k - small * series
    wide = jnp.where(small < 0.05, small * series, jnp.log(1.0 + small))
    return jnp.maximum(value, 0.0) + wide


def both_kernel(
    cap,
    mix_hbm,
    wx_hbm,
    wy_hbm,
    ga_hbm,
    gx_hbm,
    shift_hbm,
    mix_gain_hbm,
    taps_hbm,
    logit_hbm,
    moe_hbm,
    gain_hbm,
    rt_hbm,
    rw_hbm,
    gate_hbm,
    up_hbm,
    down_hbm,
    mix_ref,
    out_ref,
    mix_gain_ref,
    taps_ref,
    logit_ref,
    gain_ref,
    rt_row,
    rw_row,
    small_sem,
    nrm,
    tok,
    xs,
    stage,
    own_stage,
    picks,
    hid,
    psend,
    precv,
    pown,
    res,
    ret,
    routes_all,
    comb,
    part,
    total,
    gw,
    uw,
    w2,
    load_sem,
    rt_sem,
    z_send,
    z_recv,
    w_sem,
    x_send,
    x_recv,
    push_sem,
    ag_sem,
    rs_sem,
    ret_sem,
    mixv,
    wx,
    wy,
    gaw,
    gxw,
    shiftv,
    xb,
    yb,
    av,
    bv,
    ends,
    halo_sem,
    ends_sem,
):
    n_ep = lax.axis_size("ep")
    nz = n_ep // 2
    ep = lax.axis_index("ep")
    t = lax.axis_index("tp")
    z, c = ep // 2, ep % 2
    y, x = t // 2, t % 2
    xp, yp, dg = y * 2 + (1 - x), (1 - y) * 2 + x, 3 - t
    pa, pb = jnp.where(c == 0, xp, yp), jnp.where(c == 0, yp, xp)
    other = z * 2 + (1 - c)
    rows, share = tok.shape[2], tok.shape[3]
    inner = (z > 0) & (z + 1 < nz)
    outer = jnp.logical_not(inner)
    shares = (t, dg, xp, yp)

    def block_at(s):
        q = jnp.int32(0)
        for zz in range(nz):
            q = jnp.where(z == zz, block_order[zz][s], q)
        return q

    def remote(src, dst, send, recv, where):
        return pltpu.make_async_remote_copy(
            src_ref=src,
            dst_ref=dst,
            send_sem=send,
            recv_sem=recv,
            device_id=where,
            device_id_type=MESH,
        )

    span = w2.shape[2]
    half = w2.shape[1] // 2

    def down_rows(k):
        return down_hbm.at[0, pl.ds(pl.multiple_of(k * half, half), half)]

    loads = [
        pltpu.make_async_copy(moe_hbm, nrm, load_sem.at[0]),
        pltpu.make_async_copy(gate_hbm.at[0], gw, load_sem.at[1]),
        pltpu.make_async_copy(up_hbm.at[0], uw, load_sem.at[2]),
        pltpu.make_async_copy(mix_hbm, mixv, load_sem.at[3]),
        pltpu.make_async_copy(wx_hbm, wx, load_sem.at[4]),
        pltpu.make_async_copy(wy_hbm, wy, load_sem.at[5]),
        pltpu.make_async_copy(ga_hbm, gaw, load_sem.at[6]),
        pltpu.make_async_copy(gx_hbm, gxw, load_sem.at[7]),
        pltpu.make_async_copy(shift_hbm, shiftv, load_sem.at[8]),
        pltpu.make_async_copy(down_rows(t), w2.at[0, pl.ds(0, half)], load_sem.at[9]),
        pltpu.make_async_copy(down_rows(pa), w2.at[0, pl.ds(half, half)], load_sem.at[10]),
    ]
    small = [
        pltpu.make_async_copy(gain_hbm, gain_ref, small_sem.at[0]),
        pltpu.make_async_copy(rt_hbm, rt_row, small_sem.at[1]),
        pltpu.make_async_copy(rw_hbm, rw_row, small_sem.at[2]),
        pltpu.make_async_copy(mix_gain_hbm, mix_gain_ref, small_sem.at[3]),
        pltpu.make_async_copy(taps_hbm, taps_ref, small_sem.at[4]),
        pltpu.make_async_copy(logit_hbm, logit_ref, small_sem.at[5]),
    ]
    loads[0].start()
    for copy in small[:2]:
        copy.start()
    barrier = pltpu.get_barrier_semaphore()
    for by in range(1, n_ep):
        pl.semaphore_signal(
            barrier, inc=1, device_id={"ep": (ep + by) % n_ep}, device_id_type=MESH
        )
    for peer in (xp, yp):
        for near in (ep, other):
            pl.semaphore_signal(
                barrier, inc=1, device_id={"ep": near, "tp": peer}, device_id_type=MESH
            )
    for copy in small[2:] + loads[3:6] + loads[1:3] + loads[6:]:
        copy.start()

    def columns(k):
        return pl.ds(pl.multiple_of(k * share, share), share)

    def z_slot(q, k):
        return q * 2 + k if k < 2 else nz * 2 + k - 2

    def z_own(k, up):
        return remote(
            nrm.at[:, columns(shares[k])],
            tok.at[z, k],
            z_send.at[z],
            z_recv.at[z_slot(z, k)],
            {"ep": ep + (2 if up else -2)},
        )

    def z_copy(q, k, up):
        return remote(
            tok.at[q, k],
            tok.at[q, k],
            z_send.at[q],
            z_recv.at[z_slot(q, k)],
            {"ep": ep + (2 if up else -2)},
        )

    def route_copy(q):
        return remote(rt_row, routes_all.at[z], rt_sem.at[nz], rt_sem.at[z], {"ep": q * 2 + c})

    def w_copy(k):
        piece = half // 2
        first = (pb, dg)[k // 2] * half + k % 2 * piece
        return remote(
            down_hbm.at[0, pl.ds(pl.multiple_of(first, piece), piece)],
            w2.at[1, pl.ds(k * piece, piece)],
            w_sem.at[0],
            w_sem.at[1],
            {"tp": pb},
        )

    def xs_part(q, block, k):
        return xs.at[q, pl.ds(pl.multiple_of(block * cap, cap), cap), columns(k)]

    def x_copy(q, kind):
        to = (xp, yp, xp, yp, t, t, t, t)[kind]
        near = ep if kind < 2 else other
        src = xs_part(q, c, t) if kind < 2 else stage.at[q, max(kind - 4, 0)]
        return remote(
            src,
            xs_part(q, c, shares[max(kind - 4, 0)]),
            x_send.at[q],
            x_recv.at[q],
            {"ep": near, "tp": to},
        )

    def x_all(q, count):
        part = xs.at[q, pl.ds(0, count * cap // 4)]
        return remote(part, part, x_send.at[q], x_recv.at[q], {"ep": other})

    def own_copy(block):
        return remote(
            own_stage,
            xs.at[z, pl.ds(pl.multiple_of(block * cap, cap), cap)],
            x_send.at[z],
            x_recv.at[z],
            {"ep": other},
        )

    def ag_copy(q, cc):
        at, sem = pl.ds(cc * cap, cap), q * 2 + cc
        return remote(
            hid.at[q, at, pl.ds(0, half)],
            hid.at[q, at, pl.ds(half, half)],
            push_sem.at[0],
            ag_sem.at[sem],
            {"tp": pa},
        )

    def rs_copy(q, cc):
        at, sem = pl.ds(cc * cap, cap), q * 2 + cc
        return remote(
            psend.at[q, at], precv.at[q, at], push_sem.at[0], rs_sem.at[sem], {"tp": pb}
        )

    def ret_copy(q, cc):
        return remote(
            res.at[q, pl.ds(cc * cap, cap)],
            ret.at[ep],
            push_sem.at[1],
            ret_sem.at[ep],
            {"ep": q * 2 + cc},
        )

    def arrive(q, k):
        z_copy(q, k, 1).wait_recv()
        if k < 2:

            @pl.when((q < z) & (z + 1 < nz))
            def _():
                z_copy(q, k, 1).start()

            @pl.when((q > z) & (z > 0))
            def _():
                z_copy(q, k, 0).start()

    def make_picks(q, named):
        lane = lax.broadcasted_iota(jnp.int32, (8, rows), 0)
        which = z * 2 + jnp.where(lane == 0, c, 1 - c)
        mask = jnp.where((named[0:1] == which) | (named[1:2] == which), 1.0, 0.0)
        before = jnp.where(
            lax.broadcasted_iota(jnp.int32, (rows, rows), 0)
            < lax.broadcasted_iota(jnp.int32, (rows, rows), 1),
            1.0,
            0.0,
        ).astype(BF16)
        rank = jnp.dot(mask.astype(BF16), before, preferred_element_type=F32)
        key = jnp.where(mask > 0.5, rank, -1.0)
        seat = lax.broadcasted_iota(jnp.int32, (cap, rows), 0).astype(F32)
        for k in range(2):
            picks[q, k * cap : (k + 1) * cap] = jnp.where(
                seat == key[k : k + 1], 1.0, 0.0
            ).astype(BF16)

    def pick_own():
        for k in range(4):
            at = pl.ds(k * share, share)
            got = jnp.dot(picks[z], nrm[:, at], preferred_element_type=F32).astype(BF16)
            xs[z, pl.ds(pl.multiple_of(c * cap, cap), cap), at] = got[:cap]
            own_stage[:, at] = got[cap:]
        own_copy(c).start()

    def pick(q, k, whole=False):
        got = jnp.dot(picks[q], tok[q, k], preferred_element_type=F32).astype(BF16)
        xs[q, pl.ds(pl.multiple_of(c * cap, cap), cap), columns(shares[k])] = got[:cap]
        stage[q, k] = got[cap:]
        for kind in range(5) if k == 0 and not whole else (4 + k,):
            x_copy(q, kind).start()

    def gate_up(q):
        tile = 512

        @pl.loop(0, gw.shape[1] // tile)
        def _(j):
            cols = pl.ds(pl.multiple_of(j * tile, tile), tile)
            g = jnp.dot(xs[q], gw[:, cols], preferred_element_type=F32)
            u = jnp.dot(xs[q], uw[:, cols], preferred_element_type=F32)
            hid[q, :, cols] = (jax.nn.silu(g) * u).astype(BF16)

    def gathered(q, count=6):
        x_all(q, count).wait_recv()

    def ag_start(q):
        for cc in range(2):
            ag_copy(q, cc).start()

    def down_other(q, cc):
        tile = 512
        at = pl.ds(cc * cap, cap)
        ag_copy(q, cc).wait_recv()

        @pl.loop(0, span // tile)
        def _(j):
            cols = pl.ds(pl.multiple_of(j * tile, tile), tile)
            psend[q, at, cols] = jnp.dot(
                hid[q, at], w2[1, :, cols], preferred_element_type=F32
            ).astype(BF16)

        rs_copy(q, cc).start()

    def down_own(q):
        tile = 512

        @pl.loop(0, span // tile)
        def _(j):
            cols = pl.ds(pl.multiple_of(j * tile, tile), tile)
            pown[q, :, cols] = jnp.dot(hid[q], w2[0, :, cols], preferred_element_type=F32)

    def give(q, cc):
        at = pl.ds(cc * cap, cap)
        rs_copy(q, cc).wait_recv()
        res[q, at] = (pown[q, at] + precv[q, at].astype(F32)).astype(BF16)
        ret_copy(q, cc).start()

    def give_own():
        for cc in range(2):
            at = pl.ds(cc * cap, cap)
            rs_copy(z, cc).wait_recv()
            res[z, at] = (pown[z, at] + precv[z, at].astype(F32)).astype(BF16)

            @pl.when(c != cc)
            def _():
                ret_copy(z, cc).start()

    pad = xb.shape[0] - rows

    def halo_copy():
        return remote(
            xb.at[pl.ds(rows, pad)],
            xb.at[pl.ds(0, pad)],
            halo_sem.at[0],
            halo_sem.at[1],
            {"ep": ep + 1},
        )

    def ends_copy(by):
        return remote(
            ends.at[ep],
            ends.at[ep],
            ends_sem.at[0],
            ends_sem.at[1],
            {"ep": (ep + by) % n_ep},
        )

    def ends_all():
        part = ends.at[pl.ds(0, n_ep - 1)]
        return remote(part, part, ends_sem.at[0], ends_sem.at[1], {"ep": other})

    def norm(buffer, gain):
        strip = 64

        @pl.loop(0, rows // strip)
        def _(i):
            at = pl.ds(pl.multiple_of(i * strip, strip), strip)
            wide = buffer[at, :].astype(F32)
            scale = lax.rsqrt(jnp.mean(wide * wide, axis=-1, keepdims=True) + epsilon)
            buffer[at, :] = (wide * scale * gain[...]).astype(BF16)

    def project():
        for k in range(3, 6):
            loads[k].wait()
        norm(mixv, mix_gain_ref)
        tile = 256

        @pl.loop(0, wx.shape[1] // tile)
        def _(j):
            cols = pl.ds(pl.multiple_of(j * tile, tile), tile)
            xb[pl.ds(pad, rows), cols] = jnp.dot(
                mixv[...], wx[:, cols], preferred_element_type=F32
            ).astype(BF16)
            yb[:, cols] = jnp.dot(mixv[...], wy[:, cols], preferred_element_type=F32).astype(BF16)

        @pl.when(ep + 1 < n_ep)
        def _():
            halo_copy().start()

        @pl.when(ep == 0)
        def _():
            xb[pl.ds(0, pad), :] = jnp.zeros((pad, xb.shape[1]), BF16)

    def drives_ready():
        for k in range(6, 9):
            loads[k].wait()

        @pl.when(ep > 0)
        def _():
            halo_copy().wait_recv()

    def drives(heads):
        taps = taps_ref.shape[0]
        size = gaw.shape[1]
        for h in heads:
            cols = pl.ds(h * size, size)
            wide = xb[:, cols].astype(F32)
            conv = jnp.zeros((rows, size), F32)
            for k in range(taps):
                first_row = pad - (taps - 1) + k
                conv = conv + taps_ref[k : k + 1, cols] * wide[first_row : first_row + rows]
            x_conv = conv.astype(BF16)
            gate_a = jnp.dot(x_conv, gaw[h], preferred_element_type=F32)
            gate_x = jnp.dot(x_conv, gxw[h], preferred_element_type=F32)
            log_decay = (
                -lru_scale * jax.nn.sigmoid(gate_a) * soft_plus(-logit_ref[:, cols])
                + shiftv[:, cols]
            )
            av[:, cols] = jnp.exp(log_decay)
            bv[:, cols] = (
                jnp.sqrt(one_minus_exp(2.0 * log_decay))
                * jax.nn.sigmoid(gate_x)
                * x_conv.astype(F32)
            )

    def recur():
        width = av.shape[1]
        row = lax.broadcasted_iota(jnp.int32, (8, width), 0)

        def group(i, carry):
            at = pl.ds(pl.multiple_of(i * 8, 8), 8)
            a, b = av[at, :], bv[at, :]
            for by in (1, 2, 4):
                a_past, b_past = pltpu.roll(a, by, 0), pltpu.roll(b, by, 0)
                b = jnp.where(row >= by, a * b_past + b, b)
                a = jnp.where(row >= by, a * a_past, a)
            b = a * carry[1] + b
            a = a * carry[0]
            av[at, :] = a
            bv[at, :] = b
            return (a[7:8], b[7:8])

        through, state = lax.fori_loop(
            0, rows // 8, group, (jnp.ones((1, width), F32), jnp.zeros((1, width), F32))
        )
        ends[ep, 0:1] = through
        ends[ep, 1:2] = state
        for by in range(1, n_ep):
            ends_copy(by).start()

    def finish():
        carried = jnp.zeros((1, av.shape[1]), F32)
        ends_all().wait_recv()
        for k in range(n_ep):
            entered = ends[k, 0:1] * carried + ends[k, 1:2]
            carried = jnp.where(k < ep, entered, carried)
        strip = 32

        @pl.loop(0, rows // strip)
        def _(i):
            at = pl.ds(pl.multiple_of(i * strip, strip), strip)
            state = bv[at, :] + av[at, :] * carried
            mix_ref[at, :] = (state * jax.nn.gelu(yb[at, :].astype(F32))).astype(BF16)

    def drain_early():
        part = xs.at[0]
        remote(part, part, z_send.at[z], z_recv.at[0], {"ep": other}).wait_send()
        remote(part, part, w_sem.at[0], w_sem.at[1], {"ep": other}).wait_send()
        own_copy(c).wait_send()
        ends_all().wait_send()
        part = routes_all.at[pl.ds(0, nz - 1)]
        remote(part, part, rt_sem.at[nz], rt_sem.at[0], {"ep": other}).wait_send()

        @pl.when(ep + 1 < n_ep)
        def _():
            halo_copy().wait_send()

        def drain_one(q, carry):
            whole = inner & (q == block_at(2))

            @pl.when((q != z) & jnp.logical_not(whole))
            def _():
                x_all(q, 6).wait_send()

            @pl.when(whole)
            def _():
                x_all(q, 4).wait_send()

            @pl.when((q != z) & inner)
            def _():
                part = tok.at[q, pl.ds(0, 2)]
                remote(part, part, z_send.at[q], z_recv.at[0], {"ep": other}).wait_send()

            return carry

        lax.fori_loop(0, nz, drain_one, 0)

    def make_combine():
        weights = rw_row[...]
        sides = jnp.concatenate(
            [
                rt_row[...].astype(F32),
                weights / (weights[0:1] + weights[1:2]),
                jnp.zeros((124, rows), F32),
            ],
            axis=0,
        ).T
        one, two = sides[:, 0:1].astype(jnp.int32), sides[:, 1:2].astype(jnp.int32)
        lane = lax.broadcasted_iota(jnp.int32, (rows, 128), 1)
        mask = jnp.where((one == lane) | (two == lane), 1.0, 0.0)
        before = jnp.where(
            lax.broadcasted_iota(jnp.int32, (rows, rows), 1)
            < lax.broadcasted_iota(jnp.int32, (rows, rows), 0),
            1.0,
            0.0,
        ).astype(BF16)
        rank = jnp.dot(before, mask.astype(BF16), preferred_element_type=F32)
        key = jnp.where(mask > 0.5, rank, -1.0)
        part_one, part_two = sides[:, 2:3], sides[:, 3:4]
        seat = lax.broadcasted_iota(jnp.int32, (rows, cap), 1).astype(F32)
        for e in range(n_ep):
            comb[e] = jnp.where(seat == key[:, e : e + 1], 1.0, 0.0).astype(BF16)
            part[e] = jnp.broadcast_to(
                jnp.where(one == e, part_one, 0.0) + jnp.where(two == e, part_two, 0.0),
                (rows, 128),
            )

    def combine(e, rows_in, first=False, last=False):
        got = jnp.dot(comb[e], rows_in, preferred_element_type=F32)
        for j in range(got.shape[1] // 128):
            at = pl.ds(j * 128, 128)
            term = part[e] * got[:, j * 128 : (j + 1) * 128]
            if not first:
                term = total[:, at] + term
            if last:
                out_ref[:, at] = term.astype(BF16)
            else:
                total[:, at] = term

    def ret_wait(e):
        remote(
            res.at[0, pl.ds(0, cap)], ret.at[e], push_sem.at[1], ret_sem.at[e], {"ep": other}
        ).wait_recv()

    def combine_far(e, first=False, last=False):
        ret_wait(e)
        combine(e, ret[e], first, last)

    loads[0].wait()
    for copy in small[:2]:
        copy.wait()
    norm(nrm, gain_ref)
    pl.semaphore_wait(barrier, n_ep + 3)
    for q in range(nz):

        @pl.when(q != z)
        def _():
            route_copy(q).start()

    for k in range(4):

        @pl.when((z + 1 < nz) & ((z == 0) | (k < 2)))
        def _():
            z_own(k, 1).start()

        @pl.when((z > 0) & ((z + 1 == nz) | (k < 2)))
        def _():
            z_own(k, 0).start()

    for k in range(3):
        w_copy(k).start()
    make_picks(z, rt_row[...])
    pick_own()
    for copy in small[2:]:
        copy.wait()
    one, two, three = block_at(0), block_at(1), block_at(2)
    for q in (one, two, three):
        remote(
            rt_row, routes_all.at[q], rt_sem.at[nz], rt_sem.at[q], {"ep": q * 2 + c}
        ).wait_recv()
        make_picks(q, routes_all[q])
    project()
    own_copy(1 - c).wait_recv()
    for k in range(1, 3):
        loads[k].wait()
    gate_up(z)
    arrive(one, 0)
    pick(one, 0)
    w_copy(3).start()

    @pl.when(inner)
    def _():
        arrive(three, 0)

    make_combine()
    arrive(one, 1)
    pick(one, 1)

    @pl.when(inner)
    def _():
        arrive(three, 1)

    gathered(one)
    gate_up(one)
    ag_start(one)
    arrive(two, 0)
    pick(two, 0)
    for k in range(9, 11):
        loads[k].wait()
    remote(w2.at[1], w2.at[1], w_sem.at[0], w_sem.at[1], {"tp": pb}).wait_recv()
    down_other(one, 0)
    down_other(one, 1)
    down_own(one)
    arrive(two, 1)
    pick(two, 1)
    gathered(two)
    gate_up(two)
    ag_start(two)
    drives_ready()
    drives(range(0, 4))
    give(one, 0)
    give(one, 1)
    recur()

    @pl.when(outer)
    def _():
        arrive(three, 0)
        pick(three, 0)

    @pl.when(inner)
    def _():
        pick(three, 0, True)

    down_other(two, 0)
    ag_start(z)
    down_other(two, 1)
    down_own(two)

    @pl.when(outer)
    def _():
        arrive(three, 1)
        pick(three, 1)

    @pl.when(inner)
    def _():
        pick(three, 1)
        for k in range(2, 4):
            arrive(three, k)
            pick(three, k)


    @pl.when(outer)
    def _():
        gathered(three)

    @pl.when(inner)
    def _():
        gathered(three, 4)

    gate_up(three)
    ag_start(three)
    give(two, 0)
    give(two, 1)
    finish()
    down_other(three, 0)
    down_other(three, 1)
    down_own(three)
    down_other(z, 0)
    give(three, 0)
    down_other(z, 1)
    give(three, 1)
    down_own(z)
    give_own()
    combine_far(two * 2 + 0, first=True)
    combine_far(two * 2 + 1)
    combine(ep, res[z, pl.ds(pl.multiple_of(c * cap, cap), cap)])
    combine_far(other)
    drain_early()
    combine_far(one * 2 + 0)
    combine_far(one * 2 + 1)
    combine_far(three * 2 + 0)
    combine_far(three * 2 + 1, last=True)

    part = xs.at[pl.ds(0, 2)]
    remote(part, part, push_sem.at[0], ag_sem.at[0], {"ep": other}).wait_send()
    part = xs.at[0, pl.ds(0, (n_ep - 1) * cap // 4)]
    remote(part, part, push_sem.at[1], ag_sem.at[0], {"ep": other}).wait_send()


def hand_kernel(a_in, b_in, a_out, b_out, sem):
    copies = [
        pltpu.make_async_copy(a_in, a_out, sem.at[0]),
        pltpu.make_async_copy(b_in, b_out, sem.at[1]),
    ]
    for copy in copies:
        copy.start()
    for copy in copies:
        copy.wait()


def hand_over(a, b):
    hbm = pl.BlockSpec(memory_space=pltpu.HBM)
    vmem = pl.BlockSpec(memory_space=pltpu.VMEM)
    return pl.pallas_call(
        hand_kernel,
        out_shape=tuple(jax.ShapeDtypeStruct(v.shape, v.dtype) for v in (a, b)),
        in_specs=[vmem, vmem],
        out_specs=(hbm, hbm),
        scratch_shapes=[pltpu.SemaphoreType.DMA((2,))],
        compiler_params=pltpu.CompilerParams(vmem_limit_bytes=4 << 20),
        name="hand",
    )(a, b)


def both_fused(
    mix_in,
    mix_gain,
    w_in_x,
    w_in_y,
    conv_taps,
    recur_gate_w,
    input_gate_w,
    decay_logit,
    decay_shift,
    moe_in,
    moe_gain,
    routes,
    route_weight,
    expert_gate,
    expert_up,
    expert_down,
):
    n_ep = lax.axis_size("ep")
    nz = n_ep // 2
    rows, features = moe_in.shape
    share = features // 4
    ff_dev, out_dev = expert_gate.shape[2], expert_down.shape[2]
    width = w_in_x.shape[1]
    cap = 2 * rows * routes.shape[1] // n_ep
    pair = 2 * cap
    vmem = pl.BlockSpec(memory_space=pltpu.VMEM)
    hbm = pl.BlockSpec(memory_space=pltpu.HBM)
    dma = pltpu.SemaphoreType.DMA
    flops = 2 * n_ep * cap * features * (2 * ff_dev + out_dev)
    results = pl.pallas_call(
        functools.partial(both_kernel, cap),
        out_shape=(pltpu.VMEM((rows, width), BF16), pltpu.VMEM((rows, out_dev), BF16)),
        in_specs=[hbm] * 16,
        out_specs=(vmem, vmem),
        scratch_shapes=[
            pltpu.VMEM((1, features), F32),
            pltpu.VMEM(conv_taps.shape, F32),
            pltpu.VMEM((1, width), F32),
            pltpu.VMEM((1, features), F32),
            pltpu.VMEM(routes.shape[::-1], jnp.int32),
            pltpu.VMEM(routes.shape[::-1], F32),
            dma((6,)),
            pltpu.VMEM((rows, features), BF16),
            pltpu.VMEM((nz, 4, rows, share), BF16),
            pltpu.VMEM((nz, pair, features), BF16),
            pltpu.VMEM((nz, 4, cap, share), BF16),
            pltpu.VMEM((cap, features), BF16),
            pltpu.VMEM((nz, pair, rows), BF16),
            pltpu.VMEM((nz, pair, 2 * ff_dev), BF16),
            pltpu.VMEM((nz, pair, out_dev), BF16),
            pltpu.VMEM((nz, pair, out_dev), BF16),
            pltpu.VMEM((nz, pair, out_dev), F32),
            pltpu.VMEM((nz, pair, out_dev), BF16),
            pltpu.VMEM((n_ep, cap, out_dev), BF16),
            pltpu.VMEM((nz, 2, rows), jnp.int32),
            pltpu.VMEM((n_ep, rows, cap), BF16),
            pltpu.VMEM((n_ep, rows, 128), F32),
            pltpu.VMEM((rows, out_dev), F32),
            pltpu.VMEM(expert_gate.shape[1:], BF16),
            pltpu.VMEM(expert_up.shape[1:], BF16),
            pltpu.VMEM((2, 2 * ff_dev, out_dev), BF16),
            dma((11,)),
            dma((nz + 1,)),
            dma((nz,)),
            dma((2 * nz + 2,)),
            dma((2,)),
            dma((nz,)),
            dma((nz,)),
            dma((2,)),
            dma((n_ep,)),
            dma((n_ep,)),
            dma((n_ep,)),
            pltpu.VMEM(mix_in.shape, BF16),
            pltpu.VMEM(w_in_x.shape, BF16),
            pltpu.VMEM(w_in_y.shape, BF16),
            pltpu.VMEM(recur_gate_w.shape, BF16),
            pltpu.VMEM(input_gate_w.shape, BF16),
            pltpu.VMEM((rows, width), F32),
            pltpu.VMEM((16 + rows, width), BF16),
            pltpu.VMEM((rows, width), BF16),
            pltpu.VMEM((rows, width), F32),
            pltpu.VMEM((rows, width), F32),
            pltpu.VMEM((n_ep, 2, width), F32),
            dma((2,)),
            dma((2,)),
        ],
        compiler_params=pltpu.CompilerParams(
            collective_id=0, has_side_effects=True, vmem_limit_bytes=66000000
        ),
        cost_estimate=pl.CostEstimate(flops=flops, bytes_accessed=16 << 20, transcendentals=0),
        name="both",
    )(
        mix_in,
        w_in_x,
        w_in_y,
        recur_gate_w,
        input_gate_w,
        decay_shift,
        mix_gain[None, :],
        conv_taps,
        decay_logit[None, :],
        moe_in,
        moe_gain[None, :],
        routes.T,
        route_weight.T,
        expert_gate,
        expert_up,
        expert_down,
    )
    return hand_over(*results)


def from_behind(value, axis, by):
    count = lax.axis_size(axis)
    pairs = [(i, i + by) for i in range(count) if 0 <= i + by < count]
    return lax.ppermute(value, axis, pairs)


def entering(value, axis, combine, identity):
    count, index = (lax.axis_size(axis), lax.axis_index(axis))
    everything = jax.tree.map(lambda part: lax.all_gather(part, axis), value)
    start = jax.tree.map(
        lambda part, zero: jnp.broadcast_to(jnp.asarray(zero, part.dtype), part.shape),
        value,
        identity,
    )

    def hop(k, before):
        reached = k < index
        new = combine(before, jax.tree.map(lambda part: part[k], everything))
        return jax.tree.map(lambda a, b: jnp.where(reached, a, b), new, before)

    return lax.fori_loop(0, count, hop, start)


def norm_rows(rows, gain):
    widened = rows.astype(jnp.float32)
    scaled = widened * lax.rsqrt(jnp.mean(widened * widened, axis=-1, keepdims=True) + epsilon)
    return (scaled * gain[None, :]).astype(jnp.bfloat16)


def link(earlier, later):
    return (earlier[0] * later[0], later[0] * earlier[1] + later[1])


def fits_fused(moe_in, routes):
    n_ep = lax.axis_size("ep")
    gathered = n_ep * moe_in.size * moe_in.dtype.itemsize
    even = n_ep == 4 * routes.shape[1] == 2 * len(block_order)
    return lax.axis_size("tp") == 4 and even and gathered <= (16 << 20)


def moe_staged(moe_in, moe_gain, routes, route_weight, expert_gate, expert_up, expert_down):
    moe_rows = norm_rows(moe_in, moe_gain)
    token_count = moe_rows.shape[0]
    feature_count = moe_rows.shape[1]
    choose_count = routes.shape[1]
    expert_count = lax.axis_size("ep")
    capacity = 2 * token_count * choose_count // expert_count
    slot_total = expert_count * capacity
    expert_ids = routes.reshape(-1)
    onehot = (expert_ids[:, None] == jnp.arange(expert_count, dtype=jnp.int32)[None, :]).astype(
        jnp.int32
    )
    slot_rank = jnp.sum(jnp.cumsum(onehot, axis=0) * onehot, axis=1) - 1
    slot_index = expert_ids * capacity + slot_rank
    token_index = jnp.repeat(jnp.arange(token_count, dtype=jnp.int32), choose_count)
    slot_owner = jnp.full((slot_total,), token_count, jnp.int32).at[slot_index].set(token_index)
    padded_rows = jnp.concatenate([moe_rows, jnp.zeros((1, feature_count), jnp.bfloat16)], axis=0)
    outgoing = padded_rows[slot_owner].reshape(expert_count, capacity, feature_count)
    column_width = feature_count // lax.axis_size("tp")
    own_columns = lax.dynamic_slice_in_dim(
        outgoing, lax.axis_index("tp") * column_width, column_width, 2
    )
    incoming = lax.all_to_all(own_columns, "ep", split_axis=0, concat_axis=0, tiled=True)
    piece = lax.all_gather(incoming, "tp", axis=2, tiled=True)
    flat_rows = piece.reshape(slot_total, piece.shape[2])
    gate_rows = expert_gate[0]
    up_rows = expert_up[0]
    gate_proj = jnp.dot(flat_rows, gate_rows, preferred_element_type=jnp.float32)
    up_proj = jnp.dot(flat_rows, up_rows, preferred_element_type=jnp.float32)
    hidden = (jax.nn.silu(gate_proj) * up_proj).astype(jnp.bfloat16)
    down_rows = expert_down[0]
    columns = jnp.dot(
        lax.all_gather(hidden, "tp", axis=1, tiled=True),
        down_rows,
        preferred_element_type=jnp.float32,
    )
    results = columns.astype(jnp.bfloat16).reshape(expert_count, capacity, expert_down.shape[2])
    returned = lax.all_to_all(results, "ep", split_axis=0, concat_axis=0, tiled=True).reshape(
        slot_total, expert_down.shape[2]
    )
    picked = (
        returned[slot_index]
        .astype(jnp.float32)
        .reshape(token_count, choose_count, expert_down.shape[2])
    )
    route_share = route_weight / jnp.sum(route_weight, axis=1, keepdims=True)
    moe_out = jnp.sum(route_share[:, :, None] * picked, axis=1).astype(jnp.bfloat16)
    return moe_out


def staged(
    mix_in,
    mix_gain,
    w_in_x,
    w_in_y,
    conv_taps,
    recur_gate_w,
    input_gate_w,
    decay_logit,
    decay_shift,
    moe_in,
    moe_gain,
    routes,
    route_weight,
    expert_gate,
    expert_up,
    expert_down,
):
    row_count = mix_in.shape[0]
    width_dev = w_in_x.shape[1]
    heads_dev = recur_gate_w.shape[0]
    block_size = recur_gate_w.shape[1]
    tap_count = conv_taps.shape[0]
    mixer_rows = norm_rows(mix_in, mix_gain)
    x_branch = jnp.dot(mixer_rows, w_in_x, preferred_element_type=jnp.float32).astype(jnp.bfloat16)
    y_branch = jnp.dot(mixer_rows, w_in_y, preferred_element_type=jnp.float32).astype(jnp.bfloat16)
    previous = from_behind(x_branch[row_count - (tap_count - 1) :], "ep", 1)
    padded = jnp.concatenate([previous, x_branch], axis=0)
    conv_sum = jnp.zeros((row_count, width_dev), jnp.float32)
    for tap_index in range(tap_count):
        conv_sum = conv_sum + conv_taps[tap_index][None, :] * padded[
            tap_index : tap_index + row_count
        ].astype(jnp.float32)
    x_conv = conv_sum.astype(jnp.bfloat16)
    heads_in = x_conv.reshape(row_count, heads_dev, block_size)
    gate_a = jnp.einsum(
        "thi,hij->thj", heads_in, recur_gate_w, preferred_element_type=jnp.float32
    ).reshape(row_count, width_dev)
    gate_x = jnp.einsum(
        "thi,hij->thj", heads_in, input_gate_w, preferred_element_type=jnp.float32
    ).reshape(row_count, width_dev)
    log_decay = (
        -lru_scale * jax.nn.sigmoid(gate_a) * jax.nn.softplus(-decay_logit)[None, :] + decay_shift
    )
    lru_drive = (
        jnp.sqrt(-jnp.expm1(2.0 * log_decay)) * jax.nn.sigmoid(gate_x) * x_conv.astype(jnp.float32)
    )
    through, local_state = lax.associative_scan(link, (jnp.exp(log_decay), lru_drive), axis=0)
    identity = (jnp.ones((width_dev,), jnp.float32), jnp.zeros((width_dev,), jnp.float32))
    carried = entering((through[row_count - 1], local_state[row_count - 1]), "ep", link, identity)
    lru_state = local_state + through * carried[1][None, :]
    mixer_out = (lru_state * jax.nn.gelu(y_branch.astype(jnp.float32))).astype(jnp.bfloat16)
    moe_out = moe_staged(
        moe_in, moe_gain, routes, route_weight, expert_gate, expert_up, expert_down
    )
    return (mixer_out, moe_out)


def local(*args):
    return (both_fused if fits_fused(args[9], args[11]) else staged)(*args)


def solution(mesh):
    placed = (
        P("ep", None),
        P(),
        P(None, "tp"),
        P(None, "tp"),
        P(None, "tp"),
        P("tp", None, None),
        P("tp", None, None),
        P("tp"),
        P("ep", "tp"),
        P("ep", None),
        P(),
        P("ep", None),
        P("ep", None),
        P("ep", None, "tp"),
        P("ep", None, "tp"),
        P("ep", None, "tp"),
    )
    return jax.shard_map(
        local, mesh=mesh, in_specs=placed, out_specs=(P("ep", "tp"), P("ep", "tp")), check_vma=False
    )
```

```python
import functools

import jax
import jax.numpy as jnp
from jax import lax
from jax.experimental import pallas as pl
from jax.experimental.pallas import tpu as pltpu
from jax.sharding import PartitionSpec as P

epsilon = 1e-06
lru_scale = 8.0
MESH = pl.DeviceIdType.MESH
F32 = jnp.float32
BF16 = jnp.bfloat16


block_order = ((1, 2, 3), (2, 3, 0), (1, 0, 3), (2, 1, 0))


def one_minus_exp(value):
    series = jnp.full_like(value, 1.0 / 9.0)
    for k in range(8, 1, -1):
        series = (1.0 + value * series) * (1.0 / k)
    series = 1.0 + value * series
    return jnp.where(value > -0.5, -value * series, 1.0 - jnp.exp(value))


def soft_plus(value):
    small = jnp.exp(-jnp.abs(value))
    series = jnp.full_like(small, 1.0 / 7.0)
    for k in range(6, 0, -1):
        series = 1.0 / k - small * series
    wide = jnp.where(small < 0.05, small * series, jnp.log(1.0 + small))
    return jnp.maximum(value, 0.0) + wide


def both_kernel(
    cap,
    mix_hbm,
    wx_hbm,
    wy_hbm,
    ga_hbm,
    gx_hbm,
    shift_hbm,
    mix_gain_hbm,
    taps_hbm,
    logit_hbm,
    moe_hbm,
    gain_hbm,
    rt_hbm,
    rw_hbm,
    gate_hbm,
    up_hbm,
    down_hbm,
    mix_ref,
    out_ref,
    mix_gain_ref,
    taps_ref,
    logit_ref,
    gain_ref,
    rt_row,
    rw_row,
    small_sem,
    nrm,
    tok,
    xs,
    stage,
    own_stage,
    picks,
    hid,
    psend,
    precv,
    pown,
    res,
    ret,
    routes_all,
    comb,
    part,
    total,
    gw,
    uw,
    w2,
    load_sem,
    rt_sem,
    z_send,
    z_recv,
    w_sem,
    x_send,
    x_recv,
    push_sem,
    ag_sem,
    rs_sem,
    ret_sem,
    mixv,
    wx,
    wy,
    gaw,
    gxw,
    shiftv,
    xb,
    yb,
    av,
    bv,
    ends,
    halo_sem,
    ends_sem,
):
    n_ep = lax.axis_size("ep")
    nz = n_ep // 2
    ep = lax.axis_index("ep")
    t = lax.axis_index("tp")
    z, c = ep // 2, ep % 2
    y, x = t // 2, t % 2
    xp, yp, dg = y * 2 + (1 - x), (1 - y) * 2 + x, 3 - t
    pa, pb = jnp.where(c == 0, xp, yp), jnp.where(c == 0, yp, xp)
    other = z * 2 + (1 - c)
    rows, share = tok.shape[2], tok.shape[3]
    inner = (z > 0) & (z + 1 < nz)
    outer = jnp.logical_not(inner)
    shares = (t, dg, xp, yp)

    def block_at(s):
        q = jnp.int32(0)
        for zz in range(nz):
            q = jnp.where(z == zz, block_order[zz][s], q)
        return q

    def remote(src, dst, send, recv, where):
        return pltpu.make_async_remote_copy(
            src_ref=src,
            dst_ref=dst,
            send_sem=send,
            recv_sem=recv,
            device_id=where,
            device_id_type=MESH,
        )

    span = w2.shape[2]
    half = w2.shape[1] // 2

    def down_rows(k):
        return down_hbm.at[0, pl.ds(pl.multiple_of(k * half, half), half)]

    loads = [
        pltpu.make_async_copy(moe_hbm, nrm, load_sem.at[0]),
        pltpu.make_async_copy(gate_hbm.at[0], gw, load_sem.at[1]),
        pltpu.make_async_copy(up_hbm.at[0], uw, load_sem.at[2]),
        pltpu.make_async_copy(mix_hbm, mixv, load_sem.at[3]),
        pltpu.make_async_copy(wx_hbm, wx, load_sem.at[4]),
        pltpu.make_async_copy(wy_hbm, wy, load_sem.at[5]),
        pltpu.make_async_copy(ga_hbm, gaw, load_sem.at[6]),
        pltpu.make_async_copy(gx_hbm, gxw, load_sem.at[7]),
        pltpu.make_async_copy(shift_hbm, shiftv, load_sem.at[8]),
        pltpu.make_async_copy(down_rows(t), w2.at[0, pl.ds(0, half)], load_sem.at[9]),
        pltpu.make_async_copy(down_rows(pa), w2.at[0, pl.ds(half, half)], load_sem.at[10]),
    ]
    small = [
        pltpu.make_async_copy(gain_hbm, gain_ref, small_sem.at[0]),
        pltpu.make_async_copy(rt_hbm, rt_row, small_sem.at[1]),
        pltpu.make_async_copy(rw_hbm, rw_row, small_sem.at[2]),
        pltpu.make_async_copy(mix_gain_hbm, mix_gain_ref, small_sem.at[3]),
        pltpu.make_async_copy(taps_hbm, taps_ref, small_sem.at[4]),
        pltpu.make_async_copy(logit_hbm, logit_ref, small_sem.at[5]),
    ]
    strip_rows = rows // 4
    strips = [
        pltpu.make_async_copy(
            moe_hbm.at[pl.ds(i * strip_rows, strip_rows)],
            nrm.at[pl.ds(i * strip_rows, strip_rows)],
            load_sem.at[0 if i == 0 else 10 + i],
        )
        for i in range(4)
    ]
    for copy in strips:
        copy.start()
    for copy in small[:2]:
        copy.start()
    barrier = pltpu.get_barrier_semaphore()
    for by in range(1, n_ep):
        pl.semaphore_signal(
            barrier, inc=1, device_id={"ep": (ep + by) % n_ep}, device_id_type=MESH
        )
    for peer in (xp, yp):
        for near in (ep, other):
            pl.semaphore_signal(
                barrier, inc=1, device_id={"ep": near, "tp": peer}, device_id_type=MESH
            )
    for copy in small[2:] + loads[3:6] + loads[1:3] + loads[6:]:
        copy.start()

    def columns(k):
        return pl.ds(pl.multiple_of(k * share, share), share)

    def z_slot(q, k):
        return q * 2 + k if k < 2 else nz * 2 + k - 2

    def z_own(k, up):
        return remote(
            nrm.at[:, columns(shares[k])],
            tok.at[z, k],
            z_send.at[z],
            z_recv.at[z_slot(z, k)],
            {"ep": ep + (2 if up else -2)},
        )

    def z_copy(q, k, up):
        return remote(
            tok.at[q, k],
            tok.at[q, k],
            z_send.at[q],
            z_recv.at[z_slot(q, k)],
            {"ep": ep + (2 if up else -2)},
        )

    def route_copy(q):
        return remote(rt_row, routes_all.at[z], rt_sem.at[nz], rt_sem.at[z], {"ep": q * 2 + c})

    def w_copy(k):
        piece = half // 2
        first = (pb, dg)[k // 2] * half + k % 2 * piece
        return remote(
            down_hbm.at[0, pl.ds(pl.multiple_of(first, piece), piece)],
            w2.at[1, pl.ds(k * piece, piece)],
            w_sem.at[0],
            w_sem.at[1],
            {"tp": pb},
        )

    def xs_part(q, block, k):
        return xs.at[q, pl.ds(pl.multiple_of(block * cap, cap), cap), columns(k)]

    def x_copy(q, kind):
        to = (xp, yp, xp, yp, t, t, t, t)[kind]
        near = ep if kind < 2 else other
        src = xs_part(q, c, t) if kind < 2 else stage.at[q, max(kind - 4, 0)]
        return remote(
            src,
            xs_part(q, c, shares[max(kind - 4, 0)]),
            x_send.at[q],
            x_recv.at[q],
            {"ep": near, "tp": to},
        )

    def x_all(q, count):
        part = xs.at[q, pl.ds(0, count * cap // 4)]
        return remote(part, part, x_send.at[q], x_recv.at[q], {"ep": other})

    def own_copy(block):
        return remote(
            own_stage,
            xs.at[z, pl.ds(pl.multiple_of(block * cap, cap), cap)],
            x_send.at[z],
            x_recv.at[z],
            {"ep": other},
        )

    def ag_copy(q, cc):
        at, sem = pl.ds(cc * cap, cap), q * 2 + cc
        return remote(
            hid.at[q, at, pl.ds(0, half)],
            hid.at[q, at, pl.ds(half, half)],
            push_sem.at[0],
            ag_sem.at[sem],
            {"tp": pa},
        )

    def rs_copy(q, cc):
        at, sem = pl.ds(cc * cap, cap), q * 2 + cc
        return remote(
            psend.at[q, at], precv.at[q, at], push_sem.at[0], rs_sem.at[sem], {"tp": pb}
        )

    def ret_copy(q, cc):
        return remote(
            res.at[q, pl.ds(cc * cap, cap)],
            ret.at[ep],
            push_sem.at[1],
            ret_sem.at[ep],
            {"ep": q * 2 + cc},
        )

    def arrive(q, k):
        z_copy(q, k, 1).wait_recv()
        if k < 2:

            @pl.when((q < z) & (z + 1 < nz))
            def _():
                z_copy(q, k, 1).start()

            @pl.when((q > z) & (z > 0))
            def _():
                z_copy(q, k, 0).start()

    def make_picks(q, named):
        lane = lax.broadcasted_iota(jnp.int32, (8, rows), 0)
        which = z * 2 + jnp.where(lane == 0, c, 1 - c)
        mask = jnp.where((named[0:1] == which) | (named[1:2] == which), 1.0, 0.0)
        before = jnp.where(
            lax.broadcasted_iota(jnp.int32, (rows, rows), 0)
            < lax.broadcasted_iota(jnp.int32, (rows, rows), 1),
            1.0,
            0.0,
        ).astype(BF16)
        rank = jnp.dot(mask.astype(BF16), before, preferred_element_type=F32)
        key = jnp.where(mask > 0.5, rank, -1.0)
        seat = lax.broadcasted_iota(jnp.int32, (cap, rows), 0).astype(F32)
        for k in range(2):
            picks[q, k * cap : (k + 1) * cap] = jnp.where(
                seat == key[k : k + 1], 1.0, 0.0
            ).astype(BF16)

    def pick_own():
        for k in range(4):
            at = pl.ds(k * share, share)
            got = jnp.dot(picks[z], nrm[:, at], preferred_element_type=F32).astype(BF16)
            xs[z, pl.ds(pl.multiple_of(c * cap, cap), cap), at] = got[:cap]
            own_stage[:, at] = got[cap:]
        own_copy(c).start()

    def pick(q, k, whole=False):
        got = jnp.dot(picks[q], tok[q, k], preferred_element_type=F32).astype(BF16)
        xs[q, pl.ds(pl.multiple_of(c * cap, cap), cap), columns(shares[k])] = got[:cap]
        stage[q, k] = got[cap:]
        for kind in range(5) if k == 0 and not whole else (4 + k,):
            x_copy(q, kind).start()

    def gate_up(q):
        tile = 512

        @pl.loop(0, gw.shape[1] // tile)
        def _(j):
            cols = pl.ds(pl.multiple_of(j * tile, tile), tile)
            g = jnp.dot(xs[q], gw[:, cols], preferred_element_type=F32)
            u = jnp.dot(xs[q], uw[:, cols], preferred_element_type=F32)
            hid[q, :, cols] = (jax.nn.silu(g) * u).astype(BF16)

    def gathered(q, count=6):
        x_all(q, count).wait_recv()

    def ag_start(q):
        for cc in range(2):
            ag_copy(q, cc).start()

    def down_other(q, cc):
        tile = 512
        at = pl.ds(cc * cap, cap)
        ag_copy(q, cc).wait_recv()

        @pl.loop(0, span // tile)
        def _(j):
            cols = pl.ds(pl.multiple_of(j * tile, tile), tile)
            psend[q, at, cols] = jnp.dot(
                hid[q, at], w2[1, :, cols], preferred_element_type=F32
            ).astype(BF16)

        rs_copy(q, cc).start()

    def down_own(q):
        tile = 512

        @pl.loop(0, span // tile)
        def _(j):
            cols = pl.ds(pl.multiple_of(j * tile, tile), tile)
            pown[q, :, cols] = jnp.dot(hid[q], w2[0, :, cols], preferred_element_type=F32)

    def give(q, cc):
        at = pl.ds(cc * cap, cap)
        rs_copy(q, cc).wait_recv()
        res[q, at] = (pown[q, at] + precv[q, at].astype(F32)).astype(BF16)
        ret_copy(q, cc).start()

    def give_own():
        for cc in range(2):
            at = pl.ds(cc * cap, cap)
            rs_copy(z, cc).wait_recv()
            res[z, at] = (pown[z, at] + precv[z, at].astype(F32)).astype(BF16)

            @pl.when(c != cc)
            def _():
                ret_copy(z, cc).start()

    pad = xb.shape[0] - rows

    def halo_copy():
        return remote(
            xb.at[pl.ds(rows, pad)],
            xb.at[pl.ds(0, pad)],
            halo_sem.at[0],
            halo_sem.at[1],
            {"ep": ep + 1},
        )

    def ends_copy(by):
        return remote(
            ends.at[ep],
            ends.at[ep],
            ends_sem.at[0],
            ends_sem.at[1],
            {"ep": (ep + by) % n_ep},
        )

    def ends_all():
        part = ends.at[pl.ds(0, n_ep - 1)]
        return remote(part, part, ends_sem.at[0], ends_sem.at[1], {"ep": other})

    def norm(buffer, gain):
        strip = 64

        @pl.loop(0, rows // strip)
        def _(i):
            at = pl.ds(pl.multiple_of(i * strip, strip), strip)
            wide = buffer[at, :].astype(F32)
            scale = lax.rsqrt(jnp.mean(wide * wide, axis=-1, keepdims=True) + epsilon)
            buffer[at, :] = (wide * scale * gain[...]).astype(BF16)

    def project():
        for k in range(3, 6):
            loads[k].wait()
        norm(mixv, mix_gain_ref)
        tile = 256

        @pl.loop(0, wx.shape[1] // tile)
        def _(j):
            cols = pl.ds(pl.multiple_of(j * tile, tile), tile)
            xb[pl.ds(pad, rows), cols] = jnp.dot(
                mixv[...], wx[:, cols], preferred_element_type=F32
            ).astype(BF16)
            yb[:, cols] = jnp.dot(mixv[...], wy[:, cols], preferred_element_type=F32).astype(BF16)

        @pl.when(ep + 1 < n_ep)
        def _():
            halo_copy().start()

        @pl.when(ep == 0)
        def _():
            xb[pl.ds(0, pad), :] = jnp.zeros((pad, xb.shape[1]), BF16)

    def drives_ready():
        for k in range(6, 9):
            loads[k].wait()

        @pl.when(ep > 0)
        def _():
            halo_copy().wait_recv()

    def drives(heads):
        taps = taps_ref.shape[0]
        size = gaw.shape[1]
        for h in heads:
            cols = pl.ds(h * size, size)
            wide = xb[:, cols].astype(F32)
            conv = jnp.zeros((rows, size), F32)
            for k in range(taps):
                first_row = pad - (taps - 1) + k
                conv = conv + taps_ref[k : k + 1, cols] * wide[first_row : first_row + rows]
            x_conv = conv.astype(BF16)
            gate_a = jnp.dot(x_conv, gaw[h], preferred_element_type=F32)
            gate_x = jnp.dot(x_conv, gxw[h], preferred_element_type=F32)
            log_decay = (
                -lru_scale * jax.nn.sigmoid(gate_a) * soft_plus(-logit_ref[:, cols])
                + shiftv[:, cols]
            )
            av[:, cols] = jnp.exp(log_decay)
            bv[:, cols] = (
                jnp.sqrt(one_minus_exp(2.0 * log_decay))
                * jax.nn.sigmoid(gate_x)
                * x_conv.astype(F32)
            )

    def recur():
        width = av.shape[1]
        row = lax.broadcasted_iota(jnp.int32, (8, width), 0)

        def group(i, carry):
            at = pl.ds(pl.multiple_of(i * 8, 8), 8)
            a, b = av[at, :], bv[at, :]
            for by in (1, 2, 4):
                a_past, b_past = pltpu.roll(a, by, 0), pltpu.roll(b, by, 0)
                b = jnp.where(row >= by, a * b_past + b, b)
                a = jnp.where(row >= by, a * a_past, a)
            b = a * carry[1] + b
            a = a * carry[0]
            av[at, :] = a
            bv[at, :] = b
            return (a[7:8], b[7:8])

        through, state = lax.fori_loop(
            0, rows // 8, group, (jnp.ones((1, width), F32), jnp.zeros((1, width), F32))
        )
        ends[ep, 0:1] = through
        ends[ep, 1:2] = state
        for by in range(1, n_ep):
            ends_copy(by).start()

    def finish():
        carried = jnp.zeros((1, av.shape[1]), F32)
        ends_all().wait_recv()
        for k in range(n_ep):
            entered = ends[k, 0:1] * carried + ends[k, 1:2]
            carried = jnp.where(k < ep, entered, carried)
        strip = 32

        @pl.loop(0, rows // strip)
        def _(i):
            at = pl.ds(pl.multiple_of(i * strip, strip), strip)
            state = bv[at, :] + av[at, :] * carried
            mix_ref[at, :] = (state * jax.nn.gelu(yb[at, :].astype(F32))).astype(BF16)

    def drain_early():
        part = xs.at[0]
        remote(part, part, z_send.at[z], z_recv.at[0], {"ep": other}).wait_send()
        remote(part, part, w_sem.at[0], w_sem.at[1], {"ep": other}).wait_send()
        own_copy(c).wait_send()
        ends_all().wait_send()
        part = routes_all.at[pl.ds(0, nz - 1)]
        remote(part, part, rt_sem.at[nz], rt_sem.at[0], {"ep": other}).wait_send()

        @pl.when(ep + 1 < n_ep)
        def _():
            halo_copy().wait_send()

        def drain_one(q, carry):
            whole = inner & (q == block_at(2))

            @pl.when((q != z) & jnp.logical_not(whole))
            def _():
                x_all(q, 6).wait_send()

            @pl.when(whole)
            def _():
                x_all(q, 4).wait_send()

            @pl.when((q != z) & inner)
            def _():
                part = tok.at[q, pl.ds(0, 2)]
                remote(part, part, z_send.at[q], z_recv.at[0], {"ep": other}).wait_send()

            return carry

        lax.fori_loop(0, nz, drain_one, 0)

    def make_combine():
        weights = rw_row[...]
        sides = jnp.concatenate(
            [
                rt_row[...].astype(F32),
                weights / (weights[0:1] + weights[1:2]),
                jnp.zeros((124, rows), F32),
            ],
            axis=0,
        ).T
        one, two = sides[:, 0:1].astype(jnp.int32), sides[:, 1:2].astype(jnp.int32)
        lane = lax.broadcasted_iota(jnp.int32, (rows, 128), 1)
        mask = jnp.where((one == lane) | (two == lane), 1.0, 0.0)
        before = jnp.where(
            lax.broadcasted_iota(jnp.int32, (rows, rows), 1)
            < lax.broadcasted_iota(jnp.int32, (rows, rows), 0),
            1.0,
            0.0,
        ).astype(BF16)
        rank = jnp.dot(before, mask.astype(BF16), preferred_element_type=F32)
        key = jnp.where(mask > 0.5, rank, -1.0)
        part_one, part_two = sides[:, 2:3], sides[:, 3:4]
        seat = lax.broadcasted_iota(jnp.int32, (rows, cap), 1).astype(F32)
        for e in range(n_ep):
            comb[e] = jnp.where(seat == key[:, e : e + 1], 1.0, 0.0).astype(BF16)
            part[e] = jnp.broadcast_to(
                jnp.where(one == e, part_one, 0.0) + jnp.where(two == e, part_two, 0.0),
                (rows, 128),
            )

    def combine(e, rows_in, first=False, last=False):
        got = jnp.dot(comb[e], rows_in, preferred_element_type=F32)
        for j in range(got.shape[1] // 128):
            at = pl.ds(j * 128, 128)
            term = part[e] * got[:, j * 128 : (j + 1) * 128]
            if not first:
                term = total[:, at] + term
            if last:
                out_ref[:, at] = term.astype(BF16)
            else:
                total[:, at] = term

    def ret_wait(e):
        remote(
            res.at[0, pl.ds(0, cap)], ret.at[e], push_sem.at[1], ret_sem.at[e], {"ep": other}
        ).wait_recv()

    def combine_far(e, first=False, last=False):
        ret_wait(e)
        combine(e, ret[e], first, last)

    for copy in small[:2]:
        copy.wait()
    for i in range(4):
        strips[i].wait()
        at = pl.ds(i * strip_rows, strip_rows)
        wide = nrm[at, :].astype(F32)
        scale = lax.rsqrt(jnp.mean(wide * wide, axis=-1, keepdims=True) + epsilon)
        nrm[at, :] = (wide * scale * gain_ref[...]).astype(BF16)
    pl.semaphore_wait(barrier, n_ep + 3)
    for q in range(nz):

        @pl.when(q != z)
        def _():
            route_copy(q).start()

    for k in range(4):

        @pl.when((z + 1 < nz) & ((z == 0) | (k < 2)))
        def _():
            z_own(k, 1).start()

        @pl.when((z > 0) & ((z + 1 == nz) | (k < 2)))
        def _():
            z_own(k, 0).start()

    for k in range(3):
        w_copy(k).start()
    make_picks(z, rt_row[...])
    pick_own()
    for copy in small[2:]:
        copy.wait()
    one, two, three = block_at(0), block_at(1), block_at(2)
    for q in (one, two, three):
        remote(
            rt_row, routes_all.at[q], rt_sem.at[nz], rt_sem.at[q], {"ep": q * 2 + c}
        ).wait_recv()
        make_picks(q, routes_all[q])
    project()
    own_copy(1 - c).wait_recv()
    for k in range(1, 3):
        loads[k].wait()
    gate_up(z)
    arrive(one, 0)
    pick(one, 0)
    w_copy(3).start()

    @pl.when(inner)
    def _():
        arrive(three, 0)

    make_combine()
    arrive(one, 1)
    pick(one, 1)

    @pl.when(inner)
    def _():
        arrive(three, 1)

    gathered(one)
    gate_up(one)
    ag_start(one)
    arrive(two, 0)
    pick(two, 0)
    for k in range(9, 11):
        loads[k].wait()
    remote(w2.at[1], w2.at[1], w_sem.at[0], w_sem.at[1], {"tp": pb}).wait_recv()
    down_other(one, 0)
    down_other(one, 1)
    down_own(one)
    arrive(two, 1)
    pick(two, 1)
    gathered(two)
    gate_up(two)
    ag_start(two)
    drives_ready()
    drives(range(0, 4))
    give(one, 0)
    give(one, 1)
    recur()

    @pl.when(outer)
    def _():
        arrive(three, 0)
        pick(three, 0)

    @pl.when(inner)
    def _():
        pick(three, 0, True)

    down_other(two, 0)
    ag_start(z)
    down_other(two, 1)
    down_own(two)

    @pl.when(outer)
    def _():
        arrive(three, 1)
        pick(three, 1)

    @pl.when(inner)
    def _():
        pick(three, 1)
        for k in range(2, 4):
            arrive(three, k)
            pick(three, k)


    @pl.when(outer)
    def _():
        gathered(three)

    @pl.when(inner)
    def _():
        gathered(three, 4)

    gate_up(three)
    ag_start(three)
    give(two, 0)
    give(two, 1)
    finish()
    down_other(three, 0)
    down_other(three, 1)
    down_own(three)
    down_other(z, 0)
    give(three, 0)
    down_other(z, 1)
    give(three, 1)
    down_own(z)
    give_own()
    combine_far(two * 2 + 0, first=True)
    combine_far(two * 2 + 1)
    combine(ep, res[z, pl.ds(pl.multiple_of(c * cap, cap), cap)])
    combine_far(other)
    drain_early()
    combine_far(one * 2 + 0)
    combine_far(one * 2 + 1)
    combine_far(three * 2 + 0)
    combine_far(three * 2 + 1, last=True)

    part = xs.at[pl.ds(0, 2)]
    remote(part, part, push_sem.at[0], ag_sem.at[0], {"ep": other}).wait_send()
    part = xs.at[0, pl.ds(0, (n_ep - 1) * cap // 4)]
    remote(part, part, push_sem.at[1], ag_sem.at[0], {"ep": other}).wait_send()


def hand_kernel(a_in, b_in, a_out, b_out, sem):
    copies = [
        pltpu.make_async_copy(a_in, a_out, sem.at[0]),
        pltpu.make_async_copy(b_in, b_out, sem.at[1]),
    ]
    for copy in copies:
        copy.start()
    for copy in copies:
        copy.wait()


def hand_over(a, b):
    hbm = pl.BlockSpec(memory_space=pltpu.HBM)
    vmem = pl.BlockSpec(memory_space=pltpu.VMEM)
    return pl.pallas_call(
        hand_kernel,
        out_shape=tuple(jax.ShapeDtypeStruct(v.shape, v.dtype) for v in (a, b)),
        in_specs=[vmem, vmem],
        out_specs=(hbm, hbm),
        scratch_shapes=[pltpu.SemaphoreType.DMA((2,))],
        compiler_params=pltpu.CompilerParams(vmem_limit_bytes=4 << 20),
        name="hand",
    )(a, b)


def both_fused(
    mix_in,
    mix_gain,
    w_in_x,
    w_in_y,
    conv_taps,
    recur_gate_w,
    input_gate_w,
    decay_logit,
    decay_shift,
    moe_in,
    moe_gain,
    routes,
    route_weight,
    expert_gate,
    expert_up,
    expert_down,
):
    n_ep = lax.axis_size("ep")
    nz = n_ep // 2
    rows, features = moe_in.shape
    share = features // 4
    ff_dev, out_dev = expert_gate.shape[2], expert_down.shape[2]
    width = w_in_x.shape[1]
    cap = 2 * rows * routes.shape[1] // n_ep
    pair = 2 * cap
    vmem = pl.BlockSpec(memory_space=pltpu.VMEM)
    hbm = pl.BlockSpec(memory_space=pltpu.HBM)
    dma = pltpu.SemaphoreType.DMA
    flops = 2 * n_ep * cap * features * (2 * ff_dev + out_dev)
    results = pl.pallas_call(
        functools.partial(both_kernel, cap),
        out_shape=(pltpu.VMEM((rows, width), BF16), pltpu.VMEM((rows, out_dev), BF16)),
        in_specs=[hbm] * 16,
        out_specs=(vmem, vmem),
        scratch_shapes=[
            pltpu.VMEM((1, features), F32),
            pltpu.VMEM(conv_taps.shape, F32),
            pltpu.VMEM((1, width), F32),
            pltpu.VMEM((1, features), F32),
            pltpu.VMEM(routes.shape[::-1], jnp.int32),
            pltpu.VMEM(routes.shape[::-1], F32),
            dma((6,)),
            pltpu.VMEM((rows, features), BF16),
            pltpu.VMEM((nz, 4, rows, share), BF16),
            pltpu.VMEM((nz, pair, features), BF16),
            pltpu.VMEM((nz, 4, cap, share), BF16),
            pltpu.VMEM((cap, features), BF16),
            pltpu.VMEM((nz, pair, rows), BF16),
            pltpu.VMEM((nz, pair, 2 * ff_dev), BF16),
            pltpu.VMEM((nz, pair, out_dev), BF16),
            pltpu.VMEM((nz, pair, out_dev), BF16),
            pltpu.VMEM((nz, pair, out_dev), F32),
            pltpu.VMEM((nz, pair, out_dev), BF16),
            pltpu.VMEM((n_ep, cap, out_dev), BF16),
            pltpu.VMEM((nz, 2, rows), jnp.int32),
            pltpu.VMEM((n_ep, rows, cap), BF16),
            pltpu.VMEM((n_ep, rows, 128), F32),
            pltpu.VMEM((rows, out_dev), F32),
            pltpu.VMEM(expert_gate.shape[1:], BF16),
            pltpu.VMEM(expert_up.shape[1:], BF16),
            pltpu.VMEM((2, 2 * ff_dev, out_dev), BF16),
            dma((14,)),
            dma((nz + 1,)),
            dma((nz,)),
            dma((2 * nz + 2,)),
            dma((2,)),
            dma((nz,)),
            dma((nz,)),
            dma((2,)),
            dma((n_ep,)),
            dma((n_ep,)),
            dma((n_ep,)),
            pltpu.VMEM(mix_in.shape, BF16),
            pltpu.VMEM(w_in_x.shape, BF16),
            pltpu.VMEM(w_in_y.shape, BF16),
            pltpu.VMEM(recur_gate_w.shape, BF16),
            pltpu.VMEM(input_gate_w.shape, BF16),
            pltpu.VMEM((rows, width), F32),
            pltpu.VMEM((16 + rows, width), BF16),
            pltpu.VMEM((rows, width), BF16),
            pltpu.VMEM((rows, width), F32),
            pltpu.VMEM((rows, width), F32),
            pltpu.VMEM((n_ep, 2, width), F32),
            dma((2,)),
            dma((2,)),
        ],
        compiler_params=pltpu.CompilerParams(
            collective_id=0, has_side_effects=True, vmem_limit_bytes=66000000
        ),
        cost_estimate=pl.CostEstimate(flops=flops, bytes_accessed=16 << 20, transcendentals=0),
        name="both",
    )(
        mix_in,
        w_in_x,
        w_in_y,
        recur_gate_w,
        input_gate_w,
        decay_shift,
        mix_gain[None, :],
        conv_taps,
        decay_logit[None, :],
        moe_in,
        moe_gain[None, :],
        routes.T,
        route_weight.T,
        expert_gate,
        expert_up,
        expert_down,
    )
    return hand_over(*results)


def from_behind(value, axis, by):
    count = lax.axis_size(axis)
    pairs = [(i, i + by) for i in range(count) if 0 <= i + by < count]
    return lax.ppermute(value, axis, pairs)


def entering(value, axis, combine, identity):
    count, index = (lax.axis_size(axis), lax.axis_index(axis))
    everything = jax.tree.map(lambda part: lax.all_gather(part, axis), value)
    start = jax.tree.map(
        lambda part, zero: jnp.broadcast_to(jnp.asarray(zero, part.dtype), part.shape),
        value,
        identity,
    )

    def hop(k, before):
        reached = k < index
        new = combine(before, jax.tree.map(lambda part: part[k], everything))
        return jax.tree.map(lambda a, b: jnp.where(reached, a, b), new, before)

    return lax.fori_loop(0, count, hop, start)


def norm_rows(rows, gain):
    widened = rows.astype(jnp.float32)
    scaled = widened * lax.rsqrt(jnp.mean(widened * widened, axis=-1, keepdims=True) + epsilon)
    return (scaled * gain[None, :]).astype(jnp.bfloat16)


def link(earlier, later):
    return (earlier[0] * later[0], later[0] * earlier[1] + later[1])


def fits_fused(moe_in, routes):
    n_ep = lax.axis_size("ep")
    gathered = n_ep * moe_in.size * moe_in.dtype.itemsize
    even = n_ep == 4 * routes.shape[1] == 2 * len(block_order)
    return lax.axis_size("tp") == 4 and even and gathered <= (16 << 20)


def moe_staged(moe_in, moe_gain, routes, route_weight, expert_gate, expert_up, expert_down):
    moe_rows = norm_rows(moe_in, moe_gain)
    token_count = moe_rows.shape[0]
    feature_count = moe_rows.shape[1]
    choose_count = routes.shape[1]
    expert_count = lax.axis_size("ep")
    capacity = 2 * token_count * choose_count // expert_count
    slot_total = expert_count * capacity
    expert_ids = routes.reshape(-1)
    onehot = (expert_ids[:, None] == jnp.arange(expert_count, dtype=jnp.int32)[None, :]).astype(
        jnp.int32
    )
    slot_rank = jnp.sum(jnp.cumsum(onehot, axis=0) * onehot, axis=1) - 1
    slot_index = expert_ids * capacity + slot_rank
    token_index = jnp.repeat(jnp.arange(token_count, dtype=jnp.int32), choose_count)
    slot_owner = jnp.full((slot_total,), token_count, jnp.int32).at[slot_index].set(token_index)
    padded_rows = jnp.concatenate([moe_rows, jnp.zeros((1, feature_count), jnp.bfloat16)], axis=0)
    outgoing = padded_rows[slot_owner].reshape(expert_count, capacity, feature_count)
    column_width = feature_count // lax.axis_size("tp")
    own_columns = lax.dynamic_slice_in_dim(
        outgoing, lax.axis_index("tp") * column_width, column_width, 2
    )
    incoming = lax.all_to_all(own_columns, "ep", split_axis=0, concat_axis=0, tiled=True)
    piece = lax.all_gather(incoming, "tp", axis=2, tiled=True)
    flat_rows = piece.reshape(slot_total, piece.shape[2])
    gate_rows = expert_gate[0]
    up_rows = expert_up[0]
    gate_proj = jnp.dot(flat_rows, gate_rows, preferred_element_type=jnp.float32)
    up_proj = jnp.dot(flat_rows, up_rows, preferred_element_type=jnp.float32)
    hidden = (jax.nn.silu(gate_proj) * up_proj).astype(jnp.bfloat16)
    down_rows = expert_down[0]
    columns = jnp.dot(
        lax.all_gather(hidden, "tp", axis=1, tiled=True),
        down_rows,
        preferred_element_type=jnp.float32,
    )
    results = columns.astype(jnp.bfloat16).reshape(expert_count, capacity, expert_down.shape[2])
    returned = lax.all_to_all(results, "ep", split_axis=0, concat_axis=0, tiled=True).reshape(
        slot_total, expert_down.shape[2]
    )
    picked = (
        returned[slot_index]
        .astype(jnp.float32)
        .reshape(token_count, choose_count, expert_down.shape[2])
    )
    route_share = route_weight / jnp.sum(route_weight, axis=1, keepdims=True)
    moe_out = jnp.sum(route_share[:, :, None] * picked, axis=1).astype(jnp.bfloat16)
    return moe_out


def staged(
    mix_in,
    mix_gain,
    w_in_x,
    w_in_y,
    conv_taps,
    recur_gate_w,
    input_gate_w,
    decay_logit,
    decay_shift,
    moe_in,
    moe_gain,
    routes,
    route_weight,
    expert_gate,
    expert_up,
    expert_down,
):
    row_count = mix_in.shape[0]
    width_dev = w_in_x.shape[1]
    heads_dev = recur_gate_w.shape[0]
    block_size = recur_gate_w.shape[1]
    tap_count = conv_taps.shape[0]
    mixer_rows = norm_rows(mix_in, mix_gain)
    x_branch = jnp.dot(mixer_rows, w_in_x, preferred_element_type=jnp.float32).astype(jnp.bfloat16)
    y_branch = jnp.dot(mixer_rows, w_in_y, preferred_element_type=jnp.float32).astype(jnp.bfloat16)
    previous = from_behind(x_branch[row_count - (tap_count - 1) :], "ep", 1)
    padded = jnp.concatenate([previous, x_branch], axis=0)
    conv_sum = jnp.zeros((row_count, width_dev), jnp.float32)
    for tap_index in range(tap_count):
        conv_sum = conv_sum + conv_taps[tap_index][None, :] * padded[
            tap_index : tap_index + row_count
        ].astype(jnp.float32)
    x_conv = conv_sum.astype(jnp.bfloat16)
    heads_in = x_conv.reshape(row_count, heads_dev, block_size)
    gate_a = jnp.einsum(
        "thi,hij->thj", heads_in, recur_gate_w, preferred_element_type=jnp.float32
    ).reshape(row_count, width_dev)
    gate_x = jnp.einsum(
        "thi,hij->thj", heads_in, input_gate_w, preferred_element_type=jnp.float32
    ).reshape(row_count, width_dev)
    log_decay = (
        -lru_scale * jax.nn.sigmoid(gate_a) * jax.nn.softplus(-decay_logit)[None, :] + decay_shift
    )
    lru_drive = (
        jnp.sqrt(-jnp.expm1(2.0 * log_decay)) * jax.nn.sigmoid(gate_x) * x_conv.astype(jnp.float32)
    )
    through, local_state = lax.associative_scan(link, (jnp.exp(log_decay), lru_drive), axis=0)
    identity = (jnp.ones((width_dev,), jnp.float32), jnp.zeros((width_dev,), jnp.float32))
    carried = entering((through[row_count - 1], local_state[row_count - 1]), "ep", link, identity)
    lru_state = local_state + through * carried[1][None, :]
    mixer_out = (lru_state * jax.nn.gelu(y_branch.astype(jnp.float32))).astype(jnp.bfloat16)
    moe_out = moe_staged(
        moe_in, moe_gain, routes, route_weight, expert_gate, expert_up, expert_down
    )
    return (mixer_out, moe_out)


def local(*args):
    return (both_fused if fits_fused(args[9], args[11]) else staged)(*args)


def solution(mesh):
    placed = (
        P("ep", None),
        P(),
        P(None, "tp"),
        P(None, "tp"),
        P(None, "tp"),
        P("tp", None, None),
        P("tp", None, None),
        P("tp"),
        P("ep", "tp"),
        P("ep", None),
        P(),
        P("ep", None),
        P("ep", None),
        P("ep", None, "tp"),
        P("ep", None, "tp"),
        P("ep", None, "tp"),
    )
    return jax.shard_map(
        local, mesh=mesh, in_specs=placed, out_specs=(P("ep", "tp"), P("ep", "tp")), check_vma=False
    )
```
